32 devices in a mesh: sp: 16 (over z, y, core), tp: 2 (over x).
Axes of the slice: x: 2, y: 2, z: 4, core: 2. Of those that a mesh axis runs over, the one named last changes fastest.
Arguments:
- queries: bfloat16 [3072, 1024], P('sp', 'tp'), may hold values from -6 to 6
- keys: bfloat16 [3072, 512], P('sp', 'tp'), may hold values from -6 to 6
- values: bfloat16 [3072, 512], P('sp', 'tp'), may hold values from -6 to 6
- q_gain: float32 [64], replicated, may hold values from 0.1 to 6.5
- k_gain: float32 [64], replicated, may hold values from 0.1 to 6.5
- w_out: bfloat16 [1024, 2048], P('tp'), may hold values from -12 to 12
- residual: bfloat16 [3072, 2048], P(('sp', 'tp')), may hold values from -6 to 6
- norm_gain: float32 [2048], replicated, may hold values from 0.1 to 1.9
- w_gate: bfloat16 [2048, 5632], P('sp', 'tp'), may hold values from -0.125 to 0.125
- w_up: bfloat16 [2048, 5632], P('sp', 'tp'), may hold values from -0.125 to 0.125
- w_down: bfloat16 [5632, 2048], P('tp', 'sp'), may hold values from -0.25 to 0.25
Outputs:
- layer_out: bfloat16 [3072, 2048], P(('sp', 'tp'))
The draws below stay inside these ranges and needn't reach their ends.
All inputs are finite; a program needn't handle non-finite values.
Results may differ from the reference program's by a relative error of at most 0.018.
The reference program's roundings to bfloat16 on the way count: a program that leaves them out, or rounds other values in their place, can miss the bound.
Values may be sent and summed in bfloat16 or wider, within the bound.
A program may use at most 128 MiB of HBM per device.

```python
import math
import jax
import jax.numpy as jnp
from jax import lax

D = 2048
FF = 5632
HEADS = 16
KV_HEADS = 8
HEAD = 64
GRID_W = 128
TOKENS = 3072
ATTN = 1024
KV_WIDTH = 512


def draw_queries(key, part):
    base = jnp.clip(jax.random.normal(jax.random.fold_in(key, 11), (TOKENS, HEADS * HEAD), jnp.float32), -6.0, 6.0)
    return base.astype(jnp.bfloat16)


def draw_keys(key, part):
    base = jnp.clip(jax.random.normal(jax.random.fold_in(key, 23), (TOKENS, KV_HEADS * HEAD), jnp.float32), -6.0, 6.0)
    return base.astype(jnp.bfloat16)


def draw_q_gain(key, part):
    return jax.random.uniform(jax.random.fold_in(key, 53), (HEAD,), jnp.float32, 0.1, 1.9)


def draw_k_gain(key, part):
    return jax.random.uniform(jax.random.fold_in(key, 63), (HEAD,), jnp.float32, 0.1, 1.9)


def draw_w_out(key, part):
    base = jax.random.normal(jax.random.fold_in(key, 71), (HEADS * HEAD, D), jnp.float32)
    return jnp.clip(base * 2.0, -12.0, 12.0).astype(jnp.bfloat16)


def steps_of(stream_key, shape, cuts, least, largest):
    def one(axis_at, blocks):
        steps = jax.random.uniform(jax.random.fold_in(jax.random.fold_in(stream_key, 6), axis_at), (blocks,), jnp.float32, least / len(cuts), largest / len(cuts))
        return jnp.repeat(jnp.exp(steps), shape[axis_at] // blocks).reshape((-1,) + (1,) * (len(shape) - axis_at - 1))

    factor_of = one(*cuts[0])
    for cut in cuts[1:]:
        factor_of = factor_of * one(*cut)
    return factor_of


def centred(rng, shape, spread, limit, shards=(), held_as=jnp.bfloat16):
    factor_of = steps_of(rng, shape, shards, -0.22, 0.18) if shards else 1.0
    array = jax.random.normal(rng, shape, jnp.float32) * spread * factor_of
    return jnp.minimum(jnp.maximum(array, -limit), limit).astype(held_as)


def setup_inputs(seed: int = 0) -> dict:
    splits = jax.random.split(jax.random.key(seed), 12)
    return {
        "queries": draw_queries(jax.random.fold_in(splits[11], 71), 0),
        "keys": draw_keys(jax.random.fold_in(splits[11], 71), 0),
        "values": centred(splits[2], (TOKENS, KV_WIDTH), 1.0, 6.0, ((0, 16), (1, 2))),
        "q_gain": draw_q_gain(jax.random.fold_in(splits[11], 71), 0),
        "k_gain": draw_k_gain(jax.random.fold_in(splits[11], 71), 0),
        "w_out": draw_w_out(jax.random.fold_in(splits[11], 71), 0),
        "residual": centred(splits[6], (TOKENS, D), 1.0, 6.0, ((0, 32),)),
        "norm_gain": jnp.clip(1.0 + 0.18 * jax.random.normal(splits[7], (D,), jnp.float32), 0.1, 1.9),
        "w_gate": centred(splits[8], (D, FF), D ** -0.5, 0.125, ((0, 16), (1, 2))),
        "w_up": centred(splits[9], (D, FF), D ** -0.5, 0.125, ((0, 16), (1, 2))),
        "w_down": centred(splits[10], (FF, D), (FF // 9) ** -0.5, 0.25, ((0, 2), (1, 16))),
    }


EPS = 1e-06
THETA = 10000.0

def turn_half(part, angle):
    quarter = part.shape[-1] // 2
    cos_table = jnp.cos(angle)[:, None, :]
    sin_table = jnp.sin(angle)[:, None, :]
    first_part = part[..., :quarter]
    second_part = part[..., quarter:]
    return jnp.concatenate([first_part * cos_table - second_part * sin_table, first_part * sin_table + second_part * cos_table], axis=-1)

def head_norm_rope(flat, gain, offset, head_count):
    tok_rows = flat.shape[0]
    head_size = flat.shape[1] // head_count
    heads = flat.astype(jnp.float32).reshape(tok_rows, head_count, head_size)
    heads = heads * lax.rsqrt(lax.optimization_barrier(jnp.mean(heads * heads, axis=-1, keepdims=True)) + EPS) * gain.astype(jnp.float32)
    positions = offset + jnp.arange(tok_rows, dtype=jnp.int32)
    row_pos = (positions // GRID_W).astype(jnp.float32)
    col_pos = (positions % GRID_W).astype(jnp.float32)
    half_size = head_size // 2
    inv_freq = THETA ** (-jnp.arange(0, half_size, 2, dtype=jnp.float32) / half_size)
    turned = jnp.concatenate([turn_half(heads[..., :half_size], row_pos[:, None] * inv_freq[None, :]), turn_half(heads[..., half_size:], col_pos[:, None] * inv_freq[None, :])], axis=-1)
    return turned.reshape(tok_rows, head_count * head_size).astype(jnp.bfloat16)

def reference(queries, keys, values, q_gain, k_gain, w_out, residual, norm_gain, w_gate, w_up, w_down):
    q_group = HEADS // KV_HEADS
    q_rot = head_norm_rope(queries, q_gain, 0, HEADS)
    k_rot = head_norm_rope(keys, k_gain, 0, KV_HEADS)
    key_heads = k_rot.reshape(TOKENS, KV_HEADS, HEAD).astype(jnp.float32)
    value_heads = values.reshape(TOKENS, KV_HEADS, HEAD).astype(jnp.float32)
    block_len = math.gcd(TOKENS, 256)
    query_blocks = q_rot.reshape(TOKENS // block_len, block_len, KV_HEADS, q_group, HEAD)
    score_scale = HEAD ** (-0.5)

    def attend_block(query_block):
        scores = jnp.einsum('qhgd,khd->hgqk', query_block.astype(jnp.float32), key_heads) * score_scale
        top = lax.optimization_barrier(jnp.max(scores, axis=-1, keepdims=True))
        weights = jnp.exp(scores - top)
        totals = lax.optimization_barrier(jnp.sum(weights, axis=-1))
        rounded = weights.astype(jnp.bfloat16).astype(jnp.float32)
        mixed = jnp.einsum('hgqk,khd->qhgd', rounded, value_heads)
        mixed = mixed / jnp.transpose(totals, (2, 0, 1))[..., None]
        return mixed.astype(jnp.bfloat16).reshape(block_len, ATTN)
    attn = lax.map(attend_block, query_blocks).reshape(TOKENS, ATTN)
    proj = jnp.dot(attn, w_out, preferred_element_type=jnp.float32)
    mid = residual.astype(jnp.float32) + proj
    normed = (mid * lax.rsqrt(lax.optimization_barrier(jnp.mean(mid * mid, axis=-1, keepdims=True)) + EPS) * norm_gain.astype(jnp.float32)).astype(jnp.bfloat16)
    gate = jnp.dot(normed, w_gate, preferred_element_type=jnp.float32)
    up_part = jnp.dot(normed, w_up, preferred_element_type=jnp.float32)
    hidden = (jax.nn.silu(gate) * up_part).astype(jnp.bfloat16)
    down = jnp.dot(hidden, w_down, preferred_element_type=jnp.float32)
    return (mid + 0.5 * down).astype(jnp.bfloat16)
```

```python
import functools
import math

import jax
import jax.numpy as jnp
from jax import lax
from jax.experimental import pallas as pl
from jax.experimental.pallas import tpu as pltpu
from jax.sharding import PartitionSpec as P

GRID_W = 128


EPS = 1e-06
THETA = 10000.0


def turn_half(part, angle):
    quarter = part.shape[-1] // 2
    cos_table = jnp.cos(angle)[:, None, :]
    sin_table = jnp.sin(angle)[:, None, :]
    first_part = part[..., :quarter]
    second_part = part[..., quarter:]
    return jnp.concatenate(
        [
            first_part * cos_table - second_part * sin_table,
            first_part * sin_table + second_part * cos_table,
        ],
        axis=-1,
    )


def head_norm_rope(flat, gain, offset, head_count):
    tok_rows = flat.shape[0]
    head_size = flat.shape[1] // head_count
    heads = flat.astype(jnp.float32).reshape(tok_rows, head_count, head_size)
    heads = heads * lax.rsqrt(jnp.mean(heads * heads, axis=-1, keepdims=True) + EPS) * gain
    positions = offset + jnp.arange(tok_rows, dtype=jnp.int32)
    row_pos = (positions // GRID_W).astype(jnp.float32)
    col_pos = (positions % GRID_W).astype(jnp.float32)
    half_size = head_size // 2
    inv_freq = THETA ** (-jnp.arange(0, half_size, 2, dtype=jnp.float32) / half_size)
    turned = jnp.concatenate(
        [
            turn_half(heads[..., :half_size], row_pos[:, None] * inv_freq[None, :]),
            turn_half(heads[..., half_size:], col_pos[:, None] * inv_freq[None, :]),
        ],
        axis=-1,
    )
    return turned.reshape(tok_rows, head_count * head_size).astype(jnp.bfloat16)


def body(queries, keys, values, q_gain, k_gain, w_out, residual, norm_gain, w_gate, w_up, w_down):
    tok_rows = queries.shape[0]
    head_size = q_gain.shape[0]
    q_heads = queries.shape[1] // head_size
    kv_heads = keys.shape[1] // head_size
    q_group = q_heads // kv_heads
    offset = lax.axis_index("sp") * tok_rows
    q_rot = head_norm_rope(queries, q_gain, offset, q_heads)
    k_rot = head_norm_rope(keys, k_gain, offset, kv_heads)
    query_groups = q_rot.reshape(tok_rows, kv_heads, q_group, head_size)
    score_scale = head_size ** (-0.5)
    start_state = (
        jnp.full((kv_heads, q_group, tok_rows), -1e30, jnp.float32),
        jnp.zeros((kv_heads, q_group, tok_rows), jnp.float32),
        jnp.zeros((kv_heads, q_group, tok_rows, head_size), jnp.float32),
    )
    running = start_state
    key_piece = lax.all_gather(k_rot, "sp", axis=0, tiled=True)
    value_piece = lax.all_gather(values, "sp", axis=0, tiled=True)
    piece_len = key_piece.shape[0]
    block_len = math.gcd(piece_len, 512)
    blocks = piece_len // block_len
    key_blocks = key_piece.reshape(blocks, block_len, kv_heads, head_size)
    value_blocks = value_piece.reshape(blocks, block_len, kv_heads, head_size)

    def update(state, block_pair):
        prior_max, totals, accum = state
        key_block, value_block = block_pair
        scores = (
            jnp.einsum(
                "qhgd,khd->hgqk", query_groups, key_block, preferred_element_type=jnp.float32
            )
            * score_scale
        )
        new_max = jnp.maximum(prior_max, jnp.max(scores, axis=-1))
        weights = jnp.exp(scores - new_max[..., None])
        factor = jnp.exp(prior_max - new_max)
        totals = totals * factor + jnp.sum(weights, axis=-1)
        accum = accum * factor[..., None] + jnp.einsum(
            "hgqk,khd->hgqd",
            weights.astype(jnp.bfloat16),
            value_block,
            preferred_element_type=jnp.float32,
        )
        return ((new_max, totals, accum), None)

    running, unused = lax.scan(update, running, (key_blocks, value_blocks))
    final_max, totals, accum = running
    mixed = accum / totals[..., None]
    attn = (
        jnp.transpose(mixed, (2, 0, 1, 3))
        .reshape(tok_rows, q_heads * head_size)
        .astype(jnp.bfloat16)
    )
    own_rows = lax.all_to_all(attn, "tp", split_axis=0, concat_axis=1, tiled=True)
    columns = own_rows
    proj = jnp.dot(
        columns, lax.all_gather(w_out, "tp", axis=0, tiled=True), preferred_element_type=jnp.float32
    )
    mid = residual.astype(jnp.float32) + proj
    normed = (
        mid * lax.rsqrt(jnp.mean(mid * mid, axis=-1, keepdims=True) + EPS) * norm_gain
    ).astype(jnp.bfloat16)
    gathered = lax.all_gather(normed, "tp", axis=0, tiled=True)
    columns = gathered
    gate = jnp.dot(
        columns,
        lax.all_gather(w_gate, "sp", axis=0, tiled=True),
        preferred_element_type=jnp.float32,
    )
    up_part = jnp.dot(
        columns, lax.all_gather(w_up, "sp", axis=0, tiled=True), preferred_element_type=jnp.float32
    )
    hidden = (jax.nn.silu(gate) * up_part).astype(jnp.bfloat16)
    terms = jnp.dot(
        hidden, lax.all_gather(w_down, "sp", axis=1, tiled=True), preferred_element_type=jnp.float32
    )
    down = lax.psum_scatter(
        terms.astype(jnp.bfloat16), "tp", scatter_dimension=0, tiled=True
    ).astype(jnp.float32)
    return (mid + 0.5 * down).astype(jnp.bfloat16)


MESH = pl.DeviceIdType.MESH


def physical_ring(mesh):
    count = mesh.shape["sp"]
    try:
        places = [(tuple(d.coords), d.core_on_chip) for d in mesh.devices[:, 0].flat]
    except AttributeError:
        return None
    if count % 4 or count < 12:
        return None
    first = places[0][0]
    depth = count // 4
    for at, (coords, core) in enumerate(places):
        chip = at // 2
        want = (first[0], first[1] + chip % 2, first[2] + chip // 2)
        if coords != want or core != at % 2:
            return None
    return depth


def rope_kernel(head_size, q_ref, k_ref, qg_ref, kg_ref, cos_ref, sin_ref, q_out, k_out):
    def one(x_ref, g_ref, out_ref, scale):
        x = x_ref[...].astype(jnp.float32)
        width = x.shape[1]
        lane = lax.broadcasted_iota(jnp.int32, (width, width), 0) // head_size
        other = lax.broadcasted_iota(jnp.int32, (width, width), 1) // head_size
        same = (lane == other).astype(jnp.float32)
        mean = jnp.dot(
            x * x, same, preferred_element_type=jnp.float32, precision=lax.Precision.HIGHEST
        ) * (1.0 / head_size)
        h = x * lax.rsqrt(mean + EPS) * g_ref[...]
        quarter = head_size // 4
        repeats = width // cos_ref.shape[1]
        cos_table = jnp.concatenate([cos_ref[...]] * repeats, axis=1)
        sin_table = jnp.concatenate([sin_ref[...]] * repeats, axis=1)
        at = lax.broadcasted_iota(jnp.int32, x.shape, 1)
        is_first = (at // quarter) % 2 == 0
        ahead = pltpu.roll(h, width - quarter, 1)
        behind = pltpu.roll(h, quarter, 1)
        turned = h * cos_table + jnp.where(is_first, -ahead, behind) * sin_table
        out_ref[...] = (turned.astype(jnp.bfloat16) * scale).astype(jnp.bfloat16)

    one(q_ref, qg_ref, q_out, head_size ** (-0.5))
    one(k_ref, kg_ref, k_out, 1.0)


def gather_attend_kernel(
    depth,
    q_ref, kv_in, wg_in, wu_in, wd_in,
    attn_ref, wg_out, wu_out, wd_out,
    kv_all, own_sem, ring_send, ring_recv, sib_send, sib_recv,
):
    n = 2 * depth
    sp = lax.axis_index("sp")
    tp = lax.axis_index("tp")
    core = sp % 2
    z = sp // 4
    y = (sp // 2) % 2
    pos = (1 - y) * z + y * (n - 1 - z)

    def at_pos(p, c):
        p = lax.rem(p + n, n)
        yy = p // depth
        zz = (1 - yy) * p + yy * (n - 1 - p)
        return (zz * 2 + yy) * 2 + c

    sibling = (at_pos(pos, 1 - core), tp)
    toward = ((at_pos(pos + 1, core), tp), (at_pos(pos - 1, core), tp))

    barrier = pltpu.get_barrier_semaphore()
    for target in (sibling,) + toward:
        pl.semaphore_signal(barrier, inc=1, device_id=target, device_id_type=MESH)
    pl.semaphore_wait(barrier, 3)

    tok = kv_in.shape[0]
    rows = wg_in.shape[0]

    def half(size, way):
        return pl.ds(way * (size // 2), size // 2)

    def part(start, size, way):
        return pl.ds(pl.multiple_of(start * size + way * (size // 2), size // 2), size // 2)

    ins = (
        lambda way: kv_in.at[half(tok, way), :],
        lambda way: wg_in.at[half(rows, way), :],
        lambda way: wu_in.at[half(rows, way), :],
        lambda way: wd_in.at[half(wd_in.shape[0], way), :],
    )
    outs = (
        lambda o, way: kv_all.at[part(o, tok, way), :],
        lambda o, way: wg_out.at[part(o, rows, way), :],
        lambda o, way: wu_out.at[part(o, rows, way), :],
        lambda o, way: wd_out.at[o, half(wd_in.shape[0], way), :],
    )
    own_outs = (
        kv_all.at[pl.ds(pl.multiple_of(sp * tok, tok), tok), :],
        wg_out.at[pl.ds(pl.multiple_of(sp * rows, rows), rows), :],
        wu_out.at[pl.ds(pl.multiple_of(sp * rows, rows), rows), :],
        wd_out.at[sp],
    )
    own = [
        pltpu.make_async_copy(src, dst, own_sem.at[i])
        for i, (src, dst) in enumerate(zip((kv_in, wg_in, wu_in, wd_in), own_outs))
    ]

    def owner(step, way, c):
        return at_pos(pos - step if way == 0 else pos + step, c)

    def ring(kind, step, way):
        o = owner(step, way, core)
        src = ins[kind](way) if step == 0 else outs[kind](o, way)
        return pltpu.make_async_remote_copy(
            src_ref=src, dst_ref=outs[kind](o, way),
            send_sem=ring_send.at[kind, step, way], recv_sem=ring_recv.at[kind, step, way],
            device_id=toward[way], device_id_type=MESH,
        )

    def arrived(kind, step, way):
        o = owner(step + 1, way, core)
        pltpu.make_async_remote_copy(
            src_ref=outs[kind](o, way), dst_ref=outs[kind](o, way),
            send_sem=ring_send.at[kind, step, way], recv_sem=ring_recv.at[kind, step, way],
            device_id=toward[way], device_id_type=MESH,
        ).wait_recv()

    def across(kind, step, way, c):
        o = owner(step, way, c)
        src = ins[kind](way) if step == 0 else outs[kind](o, way)
        return pltpu.make_async_remote_copy(
            src_ref=src, dst_ref=outs[kind](o, way),
            send_sem=sib_send.at[kind, step, way], recv_sem=sib_recv.at[kind, step, way],
            device_id=sibling, device_id_type=MESH,
        )

    def serve(kind, step):
        for way in range(2):
            if step > 0:
                arrived(kind, step - 1, way)
            if step < n - 1:
                ring(kind, step, way).start()
            across(kind, step, way, core).start()

    def finish(kind):
        for step in range(n):
            for way in range(2):
                if step < n - 1:
                    ring(kind, step, way).wait_send()
                across(kind, step, way, core).wait_send()
                o = owner(step, way, 1 - core)
                pltpu.make_async_remote_copy(
                    src_ref=outs[kind](o, way), dst_ref=outs[kind](o, way),
                    send_sem=sib_send.at[kind, step, way], recv_sem=sib_recv.at[kind, step, way],
                    device_id=sibling, device_id_type=MESH,
                ).wait_recv()

    own[0].start()
    for step in range(n):
        serve(0, step)
        if step == n - 2:
            for kind in (1, 2, 3):
                own[kind].start()
    for kind in (1, 2, 3):
        serve(kind, 0)
    own[0].wait()
    finish(0)

    pairs, q_rows, lanes = q_ref.shape
    block = math.gcd(q_rows, 256)
    per_pair = q_rows // block

    def attend(at):
        pair, which = at // per_pair, at % per_pair
        span = slice(which * block, (which + 1) * block)
        q = q_ref[pair, span, :]
        k = kv_all[:, pair * lanes:(pair + 1) * lanes]
        v = kv_all[:, (pairs + pair) * lanes:(pairs + pair + 1) * lanes]
        scores = lax.dot_general(
            q, k, (((1,), (1,)), ((), ())), preferred_element_type=jnp.float32
        )
        weights = jnp.exp(scores - jnp.max(scores, axis=-1, keepdims=True))
        total = jnp.sum(weights, axis=-1, keepdims=True)
        mixed = jnp.dot(weights.astype(jnp.bfloat16), v, preferred_element_type=jnp.float32)
        attn_ref[pair, span, :] = (mixed / total).astype(jnp.bfloat16)

    todo = list(range(pairs * per_pair))
    for step in range(1, n):
        for kind in (1, 2, 3):
            serve(kind, step)
            if todo:
                attend(todo.pop(0))
    for at in todo:
        attend(at)
    for kind in (1, 2, 3):
        own[kind].wait()
        finish(kind)


def fast_body(depth, queries, keys, values, q_gain, k_gain, w_out, residual, norm_gain, w_gate, w_up, w_down):
    tok_rows = queries.shape[0]
    head_size = q_gain.shape[0]
    q_heads = queries.shape[1] // head_size
    kv_heads = keys.shape[1] // head_size
    q_group = q_heads // kv_heads
    n_sp = 4 * depth
    positions = lax.axis_index("sp") * tok_rows + jnp.arange(tok_rows, dtype=jnp.int32)
    half_size = head_size // 2
    inv_freq = THETA ** (-jnp.arange(0, half_size, 2, dtype=jnp.float32) / half_size)
    row_angle = (positions // GRID_W).astype(jnp.float32)[:, None] * inv_freq[None, :]
    col_angle = (positions % GRID_W).astype(jnp.float32)[:, None] * inv_freq[None, :]
    angle = jnp.concatenate([row_angle, row_angle, col_angle, col_angle] * 2, axis=1)
    cos_table, sin_table = jnp.cos(angle), jnp.sin(angle)
    q_rot, k_rot = pl.pallas_call(
        functools.partial(rope_kernel, head_size),
        out_shape=(
            jax.ShapeDtypeStruct(queries.shape, jnp.bfloat16),
            jax.ShapeDtypeStruct(keys.shape, jnp.bfloat16),
        ),
        name="rope",
    )(
        queries, keys,
        jnp.tile(q_gain, q_heads)[None, :], jnp.tile(k_gain, kv_heads)[None, :],
        cos_table, sin_table,
    )
    pairs = kv_heads // 2
    grouped = q_rot.reshape(tok_rows, pairs, 2, q_group, head_size)
    grouped = jnp.transpose(grouped, (1, 2, 3, 0, 4))
    empty = jnp.zeros_like(grouped[:, 0])
    padded = jnp.stack(
        [
            jnp.concatenate([grouped[:, 0], empty], axis=-1),
            jnp.concatenate([empty, grouped[:, 1]], axis=-1),
        ],
        axis=1,
    ).reshape(pairs, 2 * q_group * tok_rows, 2 * head_size)
    kv = jnp.concatenate([k_rot, values], axis=1)
    tokens = n_sp * tok_rows
    any_space = pl.BlockSpec(memory_space=pl.ANY)
    vmem = pl.BlockSpec(memory_space=pltpu.VMEM)
    n = 2 * depth
    attn_pad, wg_all, wu_all, wd_all = pl.pallas_call(
        functools.partial(gather_attend_kernel, depth),
        out_shape=(
            jax.ShapeDtypeStruct(padded.shape, jnp.bfloat16),
            jax.ShapeDtypeStruct((n_sp * w_gate.shape[0], w_gate.shape[1]), jnp.bfloat16),
            jax.ShapeDtypeStruct((n_sp * w_up.shape[0], w_up.shape[1]), jnp.bfloat16),
            jax.ShapeDtypeStruct((n_sp,) + w_down.shape, jnp.bfloat16),
        ),
        in_specs=[vmem, vmem, any_space, any_space, any_space],
        out_specs=(vmem, any_space, any_space, any_space),
        scratch_shapes=[
            pltpu.VMEM((tokens, kv.shape[1]), jnp.bfloat16),
            pltpu.SemaphoreType.DMA((4,)),
            pltpu.SemaphoreType.DMA((4, n - 1, 2)),
            pltpu.SemaphoreType.DMA((4, n - 1, 2)),
            pltpu.SemaphoreType.DMA((4, n, 2)),
            pltpu.SemaphoreType.DMA((4, n, 2)),
        ],
        compiler_params=pltpu.CompilerParams(
            collective_id=0, has_side_effects=True, vmem_limit_bytes=48 * 1024 * 1024
        ),
        cost_estimate=pl.CostEstimate(
            flops=150_000_000_000, bytes_accessed=80_000_000, transcendentals=0
        ),
        name="gather_attend",
    )(padded, kv, w_gate, w_up, w_down)
    parts = attn_pad.reshape(pairs, 2, q_group, tok_rows, 2, head_size)
    attn = jnp.stack([parts[:, 0, :, :, 0], parts[:, 1, :, :, 1]], axis=1)
    attn = jnp.transpose(attn, (3, 0, 1, 2, 4)).reshape(tok_rows, q_heads * head_size)
    own_rows = lax.all_to_all(attn, "tp", split_axis=0, concat_axis=1, tiled=True)
    proj = jnp.dot(
        own_rows, lax.all_gather(w_out, "tp", axis=0, tiled=True), preferred_element_type=jnp.float32
    )
    mid = residual.astype(jnp.float32) + proj
    normed = (
        mid * lax.rsqrt(jnp.mean(mid * mid, axis=-1, keepdims=True) + EPS) * norm_gain
    ).astype(jnp.bfloat16)
    columns = lax.all_gather(normed, "tp", axis=0, tiled=True)
    gate = jnp.dot(columns, wg_all, preferred_element_type=jnp.float32)
    up_part = jnp.dot(columns, wu_all, preferred_element_type=jnp.float32)
    hidden = (jax.nn.silu(gate) * up_part).astype(jnp.bfloat16)
    terms = jnp.einsum("th,nho->tno", hidden, wd_all, preferred_element_type=jnp.float32)
    terms = terms.reshape(tok_rows, -1)
    down = lax.psum_scatter(
        terms.astype(jnp.bfloat16), "tp", scatter_dimension=0, tiled=True
    ).astype(jnp.float32)
    return (mid + 0.5 * down).astype(jnp.bfloat16)


def solution(mesh):
    depth = physical_ring(mesh)
    inner = body if depth is None else functools.partial(fast_body, depth)
    return jax.shard_map(
        inner,
        mesh=mesh,
        in_specs=(
            P("sp", "tp"),
            P("sp", "tp"),
            P("sp", "tp"),
            P(),
            P(),
            P("tp", None),
            P(("sp", "tp"), None),
            P(),
            P("sp", "tp"),
            P("sp", "tp"),
            P("tp", "sp"),
        ),
        out_specs=P(("sp", "tp"), None),
        check_vma=False,
    )
```

```python
import functools
import math

import jax
import jax.numpy as jnp
from jax import lax
from jax.experimental import pallas as pl
from jax.experimental.pallas import tpu as pltpu
from jax.sharding import PartitionSpec as P

GRID_W = 128


EPS = 1e-06
THETA = 10000.0


def turn_half(part, angle):
    quarter = part.shape[-1] // 2
    cos_table = jnp.cos(angle)[:, None, :]
    sin_table = jnp.sin(angle)[:, None, :]
    first_part = part[..., :quarter]
    second_part = part[..., quarter:]
    return jnp.concatenate(
        [
            first_part * cos_table - second_part * sin_table,
            first_part * sin_table + second_part * cos_table,
        ],
        axis=-1,
    )


def head_norm_rope(flat, gain, offset, head_count):
    tok_rows = flat.shape[0]
    head_size = flat.shape[1] // head_count
    heads = flat.astype(jnp.float32).reshape(tok_rows, head_count, head_size)
    heads = heads * lax.rsqrt(jnp.mean(heads * heads, axis=-1, keepdims=True) + EPS) * gain
    positions = offset + jnp.arange(tok_rows, dtype=jnp.int32)
    row_pos = (positions // GRID_W).astype(jnp.float32)
    col_pos = (positions % GRID_W).astype(jnp.float32)
    half_size = head_size // 2
    inv_freq = THETA ** (-jnp.arange(0, half_size, 2, dtype=jnp.float32) / half_size)
    turned = jnp.concatenate(
        [
            turn_half(heads[..., :half_size], row_pos[:, None] * inv_freq[None, :]),
            turn_half(heads[..., half_size:], col_pos[:, None] * inv_freq[None, :]),
        ],
        axis=-1,
    )
    return turned.reshape(tok_rows, head_count * head_size).astype(jnp.bfloat16)


def body(queries, keys, values, q_gain, k_gain, w_out, residual, norm_gain, w_gate, w_up, w_down):
    tok_rows = queries.shape[0]
    head_size = q_gain.shape[0]
    q_heads = queries.shape[1] // head_size
    kv_heads = keys.shape[1] // head_size
    q_group = q_heads // kv_heads
    offset = lax.axis_index("sp") * tok_rows
    q_rot = head_norm_rope(queries, q_gain, offset, q_heads)
    k_rot = head_norm_rope(keys, k_gain, offset, kv_heads)
    query_groups = q_rot.reshape(tok_rows, kv_heads, q_group, head_size)
    score_scale = head_size ** (-0.5)
    start_state = (
        jnp.full((kv_heads, q_group, tok_rows), -1e30, jnp.float32),
        jnp.zeros((kv_heads, q_group, tok_rows), jnp.float32),
        jnp.zeros((kv_heads, q_group, tok_rows, head_size), jnp.float32),
    )
    running = start_state
    key_piece = lax.all_gather(k_rot, "sp", axis=0, tiled=True)
    value_piece = lax.all_gather(values, "sp", axis=0, tiled=True)
    piece_len = key_piece.shape[0]
    block_len = math.gcd(piece_len, 512)
    blocks = piece_len // block_len
    key_blocks = key_piece.reshape(blocks, block_len, kv_heads, head_size)
    value_blocks = value_piece.reshape(blocks, block_len, kv_heads, head_size)

    def update(state, block_pair):
        prior_max, totals, accum = state
        key_block, value_block = block_pair
        scores = (
            jnp.einsum(
                "qhgd,khd->hgqk", query_groups, key_block, preferred_element_type=jnp.float32
            )
            * score_scale
        )
        new_max = jnp.maximum(prior_max, jnp.max(scores, axis=-1))
        weights = jnp.exp(scores - new_max[..., None])
        factor = jnp.exp(prior_max - new_max)
        totals = totals * factor + jnp.sum(weights, axis=-1)
        accum = accum * factor[..., None] + jnp.einsum(
            "hgqk,khd->hgqd",
            weights.astype(jnp.bfloat16),
            value_block,
            preferred_element_type=jnp.float32,
        )
        return ((new_max, totals, accum), None)

    running, unused = lax.scan(update, running, (key_blocks, value_blocks))
    final_max, totals, accum = running
    mixed = accum / totals[..., None]
    attn = (
        jnp.transpose(mixed, (2, 0, 1, 3))
        .reshape(tok_rows, q_heads * head_size)
        .astype(jnp.bfloat16)
    )
    own_rows = lax.all_to_all(attn, "tp", split_axis=0, concat_axis=1, tiled=True)
    columns = own_rows
    proj = jnp.dot(
        columns, lax.all_gather(w_out, "tp", axis=0, tiled=True), preferred_element_type=jnp.float32
    )
    mid = residual.astype(jnp.float32) + proj
    normed = (
        mid * lax.rsqrt(jnp.mean(mid * mid, axis=-1, keepdims=True) + EPS) * norm_gain
    ).astype(jnp.bfloat16)
    gathered = lax.all_gather(normed, "tp", axis=0, tiled=True)
    columns = gathered
    gate = jnp.dot(
        columns,
        lax.all_gather(w_gate, "sp", axis=0, tiled=True),
        preferred_element_type=jnp.float32,
    )
    up_part = jnp.dot(
        columns, lax.all_gather(w_up, "sp", axis=0, tiled=True), preferred_element_type=jnp.float32
    )
    hidden = (jax.nn.silu(gate) * up_part).astype(jnp.bfloat16)
    terms = jnp.dot(
        hidden, lax.all_gather(w_down, "sp", axis=1, tiled=True), preferred_element_type=jnp.float32
    )
    down = lax.psum_scatter(
        terms.astype(jnp.bfloat16), "tp", scatter_dimension=0, tiled=True
    ).astype(jnp.float32)
    return (mid + 0.5 * down).astype(jnp.bfloat16)


MESH = pl.DeviceIdType.MESH


def physical_ring(mesh):
    count = mesh.shape["sp"]
    try:
        places = [(tuple(d.coords), d.core_on_chip) for d in mesh.devices[:, 0].flat]
    except AttributeError:
        return None
    if count % 4 or count < 12 or mesh.shape["tp"] != 2:
        return None
    first = places[0][0]
    depth = count // 4
    for at, (coords, core) in enumerate(places):
        chip = at // 2
        want = (first[0], first[1] + chip % 2, first[2] + chip // 2)
        if coords != want or core != at % 2:
            return None
    return depth


def rope_kernel(head_size, q_ref, k_ref, qg_ref, kg_ref, cos_ref, sin_ref, q_out, k_out):
    def one(x_ref, g_ref, out_ref, scale):
        x = x_ref[...].astype(jnp.float32)
        width = x.shape[1]
        lane = lax.broadcasted_iota(jnp.int32, (width, width), 0) // head_size
        other = lax.broadcasted_iota(jnp.int32, (width, width), 1) // head_size
        same = (lane == other).astype(jnp.float32)
        mean = jnp.dot(
            x * x, same, preferred_element_type=jnp.float32, precision=lax.Precision.HIGHEST
        ) * (1.0 / head_size)
        h = x * lax.rsqrt(mean + EPS) * g_ref[...]
        quarter = head_size // 4
        repeats = width // cos_ref.shape[1]
        cos_table = jnp.concatenate([cos_ref[...]] * repeats, axis=1)
        sin_table = jnp.concatenate([sin_ref[...]] * repeats, axis=1)
        at = lax.broadcasted_iota(jnp.int32, x.shape, 1)
        is_first = (at // quarter) % 2 == 0
        ahead = pltpu.roll(h, width - quarter, 1)
        behind = pltpu.roll(h, quarter, 1)
        turned = h * cos_table + jnp.where(is_first, -ahead, behind) * sin_table
        out_ref[...] = (turned.astype(jnp.bfloat16) * scale).astype(jnp.bfloat16)

    one(q_ref, qg_ref, q_out, head_size ** (-0.5))
    one(k_ref, kg_ref, k_out, 1.0)


def layer_kernel(
    depth, head_size,
    q_ref, kv_in, wo_ref, res_ref, gain_ref, wg_in, wu_in, wd_in,
    out_ref,
    kv_all, wg_all, wu_all, wd_all, attn, partial, partial_in, mid, normed, hidden,
    terms, kept, leaving, coming,
    own_sem, ring_send, ring_recv, sib_send, sib_recv, x_send, x_recv,
):
    n = 2 * depth
    sp = lax.axis_index("sp")
    tp = lax.axis_index("tp")
    core = sp % 2
    z = sp // 4
    y = (sp // 2) % 2
    pos = (1 - y) * z + y * (n - 1 - z)

    def at_pos(p, c):
        p = lax.rem(p + n, n)
        yy = p // depth
        zz = (1 - yy) * p + yy * (n - 1 - p)
        return (zz * 2 + yy) * 2 + c

    sibling = (at_pos(pos, 1 - core), tp)
    partner = (sp, 1 - tp)
    toward = ((at_pos(pos + 1, core), tp), (at_pos(pos - 1, core), tp))

    barrier = pltpu.get_barrier_semaphore()
    for target in (sibling, partner) + toward:
        pl.semaphore_signal(barrier, inc=1, device_id=target, device_id_type=MESH)
    pl.semaphore_wait(barrier, 4)

    tok = kv_in.shape[0]
    rows = wg_in.shape[0]
    units, lanes_down = wd_in.shape
    KV, GATE, UP, LOW, HIGH = range(5)

    def half(size, way, base=0):
        return pl.ds(base + way * (size // 2), size // 2)

    def part(start, size, way):
        return pl.ds(pl.multiple_of(start * size + way * (size // 2), size // 2), size // 2)

    def columns(o):
        return pl.ds(pl.multiple_of(o * lanes_down, lanes_down), lanes_down)

    ins = (
        lambda way: kv_in.at[half(tok, way), :],
        lambda way: wg_in.at[half(rows, way), :],
        lambda way: wu_in.at[half(rows, way), :],
        lambda way: wd_in.at[half(units // 2, way), :],
        lambda way: wd_in.at[half(units // 2, way, units // 2), :],
    )
    outs = (
        lambda o, way: kv_all.at[part(o, tok, way), :],
        lambda o, way: wg_all.at[part(o, rows, way), :],
        lambda o, way: wu_all.at[part(o, rows, way), :],
        lambda o, way: wd_all.at[half(units // 2, way), columns(o)],
        lambda o, way: wd_all.at[half(units // 2, way, units // 2), columns(o)],
    )
    own_outs = (
        kv_all.at[pl.ds(pl.multiple_of(sp * tok, tok), tok), :],
        wg_all.at[pl.ds(pl.multiple_of(sp * rows, rows), rows), :],
        wu_all.at[pl.ds(pl.multiple_of(sp * rows, rows), rows), :],
        wd_all.at[:, columns(sp)],
    )
    own = [
        pltpu.make_async_copy(src, dst, own_sem.at[i])
        for i, (src, dst) in enumerate(zip((kv_in, wg_in, wu_in, wd_in), own_outs))
    ]

    def owner(step, way, c):
        return at_pos(pos - step if way == 0 else pos + step, c)

    def remote(src, dst, send_sem, recv_sem, target):
        return pltpu.make_async_remote_copy(
            src_ref=src, dst_ref=dst, send_sem=send_sem, recv_sem=recv_sem,
            device_id=target, device_id_type=MESH,
        )

    def ring(kind, step, way):
        o = owner(step, way, core)
        src = ins[kind](way) if step == 0 else outs[kind](o, way)
        return remote(
            src, outs[kind](o, way),
            ring_send.at[kind, step, way], ring_recv.at[kind, step, way], toward[way],
        )

    def arrived(kind, step, way):
        piece = outs[kind](owner(step + 1, way, core), way)
        remote(
            piece, piece,
            ring_send.at[kind, step, way], ring_recv.at[kind, step, way], toward[way],
        ).wait_recv()

    def across(kind, step, way):
        o = owner(step, way, core)
        src = ins[kind](way) if step == 0 else outs[kind](o, way)
        return remote(
            src, outs[kind](o, way),
            sib_send.at[kind, step, way], sib_recv.at[kind, step, way], sibling,
        )

    def serve(kind, step):
        for way in range(2):
            if step > 0:
                arrived(kind, step - 1, way)
            if step < n - 1:
                ring(kind, step, way).start()
            across(kind, step, way).start()

    def sibling_gave(kind, steps):
        for step in steps:
            for way in range(2):
                piece = outs[kind](owner(step, way, 1 - core), way)
                remote(
                    piece, piece,
                    sib_send.at[kind, step, way], sib_recv.at[kind, step, way], sibling,
                ).wait_recv()

    pairs, q_rows, lanes = q_ref.shape
    block = math.gcd(q_rows, 256)
    per_pair = q_rows // block

    def attend(at):
        pair, which = at // per_pair, at % per_pair
        span = slice(which * block, (which + 1) * block)
        q = q_ref[pair, span, :]
        k = kv_all[:, pair * lanes:(pair + 1) * lanes]
        v = kv_all[:, (pairs + pair) * lanes:(pairs + pair + 1) * lanes]
        scores = lax.dot_general(
            q, k, (((1,), (1,)), ((), ())), preferred_element_type=jnp.float32
        )
        weights = jnp.exp(scores - jnp.max(scores, axis=-1, keepdims=True))
        total = jnp.sum(weights, axis=-1, keepdims=True)
        mixed = jnp.dot(weights.astype(jnp.bfloat16), v, preferred_element_type=jnp.float32)
        attn[pair, span, :] = (mixed / total).astype(jnp.bfloat16)

    width = wo_ref.shape[1]

    def project():
        group = q_rows // (2 * tok)
        blocks = []
        for pair in range(pairs):
            for side in range(2):
                for g in range(0, group, 2):
                    lower = attn[pair, pl.ds((side * group + g) * tok, tok), :].astype(jnp.float32)
                    upper = attn[pair, pl.ds((side * group + g + 1) * tok, tok), :].astype(jnp.float32)
                    if side == 1:
                        lower = pltpu.roll(lower, head_size, 1)
                    else:
                        upper = pltpu.roll(upper, head_size, 1)
                    lane = lax.broadcasted_iota(jnp.int32, lower.shape, 1)
                    blocks.append(jnp.where(lane < head_size, lower, upper).astype(jnp.bfloat16))
        together = jnp.concatenate(blocks, axis=1)
        wide = math.gcd(width, 512)
        for at in range(0, width, wide):
            partial[:, at:at + wide] = jnp.dot(
                together, wo_ref[:, at:at + wide], preferred_element_type=jnp.float32
            )

    own_count = res_ref.shape[0]
    mine = pl.ds(pl.multiple_of(tp * own_count, own_count), own_count)
    theirs = pl.ds(pl.multiple_of((1 - tp) * own_count, own_count), own_count)
    give_partial = remote(partial.at[theirs, :], partial_in, x_send.at[0], x_recv.at[0], partner)
    give_normed = remote(
        normed.at[mine, :], normed.at[mine, :], x_send.at[1], x_recv.at[1], partner
    )
    take_normed = remote(
        normed.at[theirs, :], normed.at[theirs, :], x_send.at[1], x_recv.at[1], partner
    )

    def normalize():
        give_partial.wait_recv()
        value = res_ref[...].astype(jnp.float32) + (partial[mine, :] + partial_in[...])
        mid[...] = value
        scale = lax.rsqrt(jnp.mean(value * value, axis=-1, keepdims=True) + EPS)
        normed[mine, :] = (value * scale * gain_ref[...]).astype(jnp.bfloat16)

    tile = math.gcd(units, 256)

    def feed(first, last):
        @pl.loop(first, last)
        def _(at):
            cols = pl.ds(pl.multiple_of(at * tile, tile), tile)
            x = normed[...]
            gate = jnp.dot(x, wg_all[:, cols], preferred_element_type=jnp.float32)
            up = jnp.dot(x, wu_all[:, cols], preferred_element_type=jnp.float32)
            hidden[:, cols] = (gate / (1.0 + jnp.exp(-gate)) * up).astype(jnp.bfloat16)

    def pair_columns(d):
        o = at_pos(pos - d, 0)
        return pl.ds(pl.multiple_of(o * lanes_down, 2 * lanes_down), 2 * lanes_down)

    def give_terms(d):
        return remote(leaving.at[d], coming.at[d], x_send.at[2 + d], x_recv.at[2 + d], partner)

    def lower(d):
        terms[...] = jnp.dot(
            hidden[...], wd_all[:, pair_columns(d)], preferred_element_type=jnp.float32
        )
        kept[d] = terms[mine, :]
        leaving[d] = terms[theirs, :].astype(jnp.bfloat16)

    def emit(d):
        give_terms(d).wait_recv()
        cols = pair_columns(d)
        down = kept[d] + coming[d].astype(jnp.float32)
        out_ref[:, cols] = (mid[:, cols] + 0.5 * down).astype(jnp.bfloat16)

    for copy in own:
        copy.start()
    early = [(kind, step) for step in range(n) for kind in (GATE, UP)]
    blocks = pairs * per_pair
    done_blocks = 0
    for slot, (kind, step) in enumerate(early):
        if slot < n:
            serve(KV, slot)
        serve(kind, step)
        if slot == n:
            own[KV].wait()
            sibling_gave(KV, range(n))
        if slot >= n:
            target = min(blocks, -(-blocks * (slot - n + 1) // (n - 2)))
            while done_blocks < target:
                attend(done_blocks)
                done_blocks += 1
        if slot == 2 * n - 2:
            project()
        if slot == 2 * n - 1:
            give_partial.start()
    tiles = units // tile
    fed = 0
    feed_from, feed_slots = 3, n - 3
    stage_of = {n // 2 + i: ([n // 2 - i, n // 2 + i] if i else [n // 2]) for i in range(n // 2)}
    waiting = []
    late = [(kind, step) for step in range(n) for kind in (LOW, HIGH)]
    for slot, (kind, step) in enumerate(late):
        serve(kind, step)
        for d in waiting:
            give_terms(d).start()
        waiting = []
        if slot == 0:
            normalize()
        if slot == 1:
            give_normed.start()
            for other in (GATE, UP):
                own[other].wait()
                sibling_gave(other, range(n))
        if slot == feed_from - 1:
            take_normed.wait_recv()
        if feed_from - 1 <= slot < n:
            target = min(tiles, -(-tiles * (slot - feed_from + 2) // (feed_slots + 1)))
            if target > fed:
                feed(fed, target)
                fed = target
        if slot == n:
            own[3].wait()
            for other in (LOW, HIGH):
                sibling_gave(other, range(1))
            lower(0)
            waiting.append(0)
        if kind == HIGH and step >= n // 2:
            fresh = range(1, step + 1) if step == n // 2 else range(step, step + 1)
            for other in (LOW, HIGH):
                sibling_gave(other, fresh)
            for d in stage_of[step]:
                lower(d)
                waiting.append(d)
    give_terms(waiting[0]).start()
    ready = [0] + [d for step in range(n // 2, n - 1) for d in stage_of[step]]
    for d in ready:
        emit(d)
    give_terms(waiting[1]).start()
    for d in waiting:
        emit(d)
    for kind in range(5):
        for step in range(n):
            for way in range(2):
                if step < n - 1:
                    ring(kind, step, way).wait_send()
                across(kind, step, way).wait_send()
    give_partial.wait_send()
    give_normed.wait_send()
    for d in range(n):
        give_terms(d).wait_send()


def fast_body(depth, queries, keys, values, q_gain, k_gain, w_out, residual, norm_gain, w_gate, w_up, w_down):
    tok_rows = queries.shape[0]
    head_size = q_gain.shape[0]
    q_heads = queries.shape[1] // head_size
    kv_heads = keys.shape[1] // head_size
    q_group = q_heads // kv_heads
    n_sp = 4 * depth
    positions = lax.axis_index("sp") * tok_rows + jnp.arange(tok_rows, dtype=jnp.int32)
    half_size = head_size // 2
    inv_freq = THETA ** (-jnp.arange(0, half_size, 2, dtype=jnp.float32) / half_size)
    row_angle = (positions // GRID_W).astype(jnp.float32)[:, None] * inv_freq[None, :]
    col_angle = (positions % GRID_W).astype(jnp.float32)[:, None] * inv_freq[None, :]
    angle = jnp.concatenate([row_angle, row_angle, col_angle, col_angle] * 2, axis=1)
    cos_table, sin_table = jnp.cos(angle), jnp.sin(angle)
    q_rot, k_rot = pl.pallas_call(
        functools.partial(rope_kernel, head_size),
        out_shape=(
            jax.ShapeDtypeStruct(queries.shape, jnp.bfloat16),
            jax.ShapeDtypeStruct(keys.shape, jnp.bfloat16),
        ),
        name="rope",
    )(
        queries, keys,
        jnp.tile(q_gain, q_heads)[None, :], jnp.tile(k_gain, kv_heads)[None, :],
        cos_table, sin_table,
    )
    pairs = kv_heads // 2
    grouped = q_rot.reshape(tok_rows, pairs, 2, q_group, head_size)
    grouped = jnp.transpose(grouped, (1, 2, 3, 0, 4))
    empty = jnp.zeros_like(grouped[:, 0])
    padded = jnp.stack(
        [
            jnp.concatenate([grouped[:, 0], empty], axis=-1),
            jnp.concatenate([empty, grouped[:, 1]], axis=-1),
        ],
        axis=1,
    ).reshape(pairs, 2 * q_group * tok_rows, 2 * head_size)
    kv = jnp.concatenate([k_rot, values], axis=1)
    tokens = n_sp * tok_rows
    any_space = pl.BlockSpec(memory_space=pl.ANY)
    vmem = pl.BlockSpec(memory_space=pltpu.VMEM)
    n = 2 * depth
    own_count, width = residual.shape
    depth_in, units = w_gate.shape
    lanes_down = w_down.shape[1]
    bf16, f32 = jnp.bfloat16, jnp.float32
    return pl.pallas_call(
        functools.partial(layer_kernel, depth, head_size),
        out_shape=jax.ShapeDtypeStruct(residual.shape, bf16),
        in_specs=[vmem] * 5 + [any_space] * 3,
        out_specs=vmem,
        scratch_shapes=[
            pltpu.VMEM((tokens, kv.shape[1]), bf16),
            pltpu.VMEM((n_sp * depth_in, units), bf16),
            pltpu.VMEM((n_sp * depth_in, units), bf16),
            pltpu.VMEM((units, n_sp * lanes_down), bf16),
            pltpu.VMEM(padded.shape, bf16),
            pltpu.VMEM((tok_rows, width), f32),
            pltpu.VMEM((own_count, width), f32),
            pltpu.VMEM((own_count, width), f32),
            pltpu.VMEM((tok_rows, width), bf16),
            pltpu.VMEM((tok_rows, units), bf16),
            pltpu.VMEM((tok_rows, 2 * lanes_down), f32),
            pltpu.VMEM((n, own_count, 2 * lanes_down), f32),
            pltpu.VMEM((n, own_count, 2 * lanes_down), bf16),
            pltpu.VMEM((n, own_count, 2 * lanes_down), bf16),
            pltpu.SemaphoreType.DMA((4,)),
            pltpu.SemaphoreType.DMA((5, n - 1, 2)),
            pltpu.SemaphoreType.DMA((5, n - 1, 2)),
            pltpu.SemaphoreType.DMA((5, n, 2)),
            pltpu.SemaphoreType.DMA((5, n, 2)),
            pltpu.SemaphoreType.DMA((2 + n,)),
            pltpu.SemaphoreType.DMA((2 + n,)),
        ],
        compiler_params=pltpu.CompilerParams(
            collective_id=0, has_side_effects=True, vmem_limit_bytes=63 * 1024 * 1024
        ),
        name="layer",
    )(padded, kv, w_out, residual, norm_gain[None, :], w_gate, w_up, w_down)


def solution(mesh):
    depth = physical_ring(mesh)
    inner = body if depth is None else functools.partial(fast_body, depth)
    return jax.shard_map(
        inner,
        mesh=mesh,
        in_specs=(
            P("sp", "tp"),
            P("sp", "tp"),
            P("sp", "tp"),
            P(),
            P(),
            P("tp", None),
            P(("sp", "tp"), None),
            P(),
            P("sp", "tp"),
            P("sp", "tp"),
            P("tp", "sp"),
        ),
        out_specs=P(("sp", "tp"), None),
        check_vma=False,
    )
```

```python
import functools
import math

import jax
import jax.numpy as jnp
from jax import lax
from jax.experimental import pallas as pl
from jax.experimental.pallas import tpu as pltpu
from jax.sharding import PartitionSpec as P

GRID_W = 128


EPS = 1e-06
THETA = 10000.0


def turn_half(part, angle):
    quarter = part.shape[-1] // 2
    cos_table = jnp.cos(angle)[:, None, :]
    sin_table = jnp.sin(angle)[:, None, :]
    first_part = part[..., :quarter]
    second_part = part[..., quarter:]
    return jnp.concatenate(
        [
            first_part * cos_table - second_part * sin_table,
            first_part * sin_table + second_part * cos_table,
        ],
        axis=-1,
    )


def head_norm_rope(flat, gain, offset, head_count):
    tok_rows = flat.shape[0]
    head_size = flat.shape[1] // head_count
    heads = flat.astype(jnp.float32).reshape(tok_rows, head_count, head_size)
    heads = heads * lax.rsqrt(jnp.mean(heads * heads, axis=-1, keepdims=True) + EPS) * gain
    positions = offset + jnp.arange(tok_rows, dtype=jnp.int32)
    row_pos = (positions // GRID_W).astype(jnp.float32)
    col_pos = (positions % GRID_W).astype(jnp.float32)
    half_size = head_size // 2
    inv_freq = THETA ** (-jnp.arange(0, half_size, 2, dtype=jnp.float32) / half_size)
    turned = jnp.concatenate(
        [
            turn_half(heads[..., :half_size], row_pos[:, None] * inv_freq[None, :]),
            turn_half(heads[..., half_size:], col_pos[:, None] * inv_freq[None, :]),
        ],
        axis=-1,
    )
    return turned.reshape(tok_rows, head_count * head_size).astype(jnp.bfloat16)


def body(queries, keys, values, q_gain, k_gain, w_out, residual, norm_gain, w_gate, w_up, w_down):
    tok_rows = queries.shape[0]
    head_size = q_gain.shape[0]
    q_heads = queries.shape[1] // head_size
    kv_heads = keys.shape[1] // head_size
    q_group = q_heads // kv_heads
    offset = lax.axis_index("sp") * tok_rows
    q_rot = head_norm_rope(queries, q_gain, offset, q_heads)
    k_rot = head_norm_rope(keys, k_gain, offset, kv_heads)
    query_groups = q_rot.reshape(tok_rows, kv_heads, q_group, head_size)
    score_scale = head_size ** (-0.5)
    start_state = (
        jnp.full((kv_heads, q_group, tok_rows), -1e30, jnp.float32),
        jnp.zeros((kv_heads, q_group, tok_rows), jnp.float32),
        jnp.zeros((kv_heads, q_group, tok_rows, head_size), jnp.float32),
    )
    running = start_state
    key_piece = lax.all_gather(k_rot, "sp", axis=0, tiled=True)
    value_piece = lax.all_gather(values, "sp", axis=0, tiled=True)
    piece_len = key_piece.shape[0]
    block_len = math.gcd(piece_len, 512)
    blocks = piece_len // block_len
    key_blocks = key_piece.reshape(blocks, block_len, kv_heads, head_size)
    value_blocks = value_piece.reshape(blocks, block_len, kv_heads, head_size)

    def update(state, block_pair):
        prior_max, totals, accum = state
        key_block, value_block = block_pair
        scores = (
            jnp.einsum(
                "qhgd,khd->hgqk", query_groups, key_block, preferred_element_type=jnp.float32
            )
            * score_scale
        )
        new_max = jnp.maximum(prior_max, jnp.max(scores, axis=-1))
        weights = jnp.exp(scores - new_max[..., None])
        factor = jnp.exp(prior_max - new_max)
        totals = totals * factor + jnp.sum(weights, axis=-1)
        accum = accum * factor[..., None] + jnp.einsum(
            "hgqk,khd->hgqd",
            weights.astype(jnp.bfloat16),
            value_block,
            preferred_element_type=jnp.float32,
        )
        return ((new_max, totals, accum), None)

    running, unused = lax.scan(update, running, (key_blocks, value_blocks))
    final_max, totals, accum = running
    mixed = accum / totals[..., None]
    attn = (
        jnp.transpose(mixed, (2, 0, 1, 3))
        .reshape(tok_rows, q_heads * head_size)
        .astype(jnp.bfloat16)
    )
    own_rows = lax.all_to_all(attn, "tp", split_axis=0, concat_axis=1, tiled=True)
    columns = own_rows
    proj = jnp.dot(
        columns, lax.all_gather(w_out, "tp", axis=0, tiled=True), preferred_element_type=jnp.float32
    )
    mid = residual.astype(jnp.float32) + proj
    normed = (
        mid * lax.rsqrt(jnp.mean(mid * mid, axis=-1, keepdims=True) + EPS) * norm_gain
    ).astype(jnp.bfloat16)
    gathered = lax.all_gather(normed, "tp", axis=0, tiled=True)
    columns = gathered
    gate = jnp.dot(
        columns,
        lax.all_gather(w_gate, "sp", axis=0, tiled=True),
        preferred_element_type=jnp.float32,
    )
    up_part = jnp.dot(
        columns, lax.all_gather(w_up, "sp", axis=0, tiled=True), preferred_element_type=jnp.float32
    )
    hidden = (jax.nn.silu(gate) * up_part).astype(jnp.bfloat16)
    terms = jnp.dot(
        hidden, lax.all_gather(w_down, "sp", axis=1, tiled=True), preferred_element_type=jnp.float32
    )
    down = lax.psum_scatter(
        terms.astype(jnp.bfloat16), "tp", scatter_dimension=0, tiled=True
    ).astype(jnp.float32)
    return (mid + 0.5 * down).astype(jnp.bfloat16)


MESH = pl.DeviceIdType.MESH


def physical_ring(mesh):
    count = mesh.shape["sp"]
    try:
        places = [(tuple(d.coords), d.core_on_chip) for d in mesh.devices[:, 0].flat]
    except AttributeError:
        return None
    if count % 4 or count < 12 or mesh.shape["tp"] != 2:
        return None
    first = places[0][0]
    depth = count // 4
    for at, (coords, core) in enumerate(places):
        chip = at // 2
        want = (first[0], first[1] + chip % 2, first[2] + chip // 2)
        if coords != want or core != at % 2:
            return None
    return depth


def rope_kernel(head_size, q_ref, k_ref, qg_ref, kg_ref, cos_ref, sin_ref, q_out, k_out):
    def one(x_ref, g_ref, out_ref, scale):
        x = x_ref[...].astype(jnp.float32)
        width = x.shape[1]
        lane = lax.broadcasted_iota(jnp.int32, (width, width), 0) // head_size
        other = lax.broadcasted_iota(jnp.int32, (width, width), 1) // head_size
        same = (lane == other).astype(jnp.float32)
        mean = jnp.dot(
            x * x, same, preferred_element_type=jnp.float32, precision=lax.Precision.HIGHEST
        ) * (1.0 / head_size)
        h = x * lax.rsqrt(mean + EPS) * jnp.concatenate([g_ref[...]] * (width // head_size), axis=1)
        quarter = head_size // 4
        repeats = width // cos_ref.shape[1]
        cos_table = jnp.concatenate([cos_ref[...]] * repeats, axis=1)
        sin_table = jnp.concatenate([sin_ref[...]] * repeats, axis=1)
        at = lax.broadcasted_iota(jnp.int32, x.shape, 1)
        is_first = (at // quarter) % 2 == 0
        ahead = pltpu.roll(h, width - quarter, 1)
        behind = pltpu.roll(h, quarter, 1)
        turned = h * cos_table + jnp.where(is_first, -ahead, behind) * sin_table
        out_ref[...] = (turned.astype(jnp.bfloat16) * scale).astype(jnp.bfloat16)

    one(q_ref, qg_ref, q_out, head_size ** (-0.5))
    one(k_ref, kg_ref, k_out, 1.0)


def layer_kernel(
    depth, head_size,
    q_ref, kv_in, res_ref, gain_ref, wo_in, wg_in, wu_in, wd_in,
    out_ref,
    kv_all, wg_all, wu_all, wd_all, wo_own, wo_other, attn, context, context_in, mid, normed, hidden,
    terms, kept, leaving, coming,
    own_sem, ring_send, ring_recv, sib_send, sib_recv, x_send, x_recv,
):
    n = 2 * depth
    sp = lax.axis_index("sp")
    tp = lax.axis_index("tp")
    core = sp % 2
    z = sp // 4
    y = (sp // 2) % 2
    pos = (1 - y) * z + y * (n - 1 - z)

    def at_pos(p, c):
        p = lax.rem(p + n, n)
        yy = p // depth
        zz = (1 - yy) * p + yy * (n - 1 - p)
        return (zz * 2 + yy) * 2 + c

    sibling = (at_pos(pos, 1 - core), tp)
    partner = (sp, 1 - tp)
    toward = ((at_pos(pos + 1, core), tp), (at_pos(pos - 1, core), tp))

    barrier = pltpu.get_barrier_semaphore()
    for target in (sibling, partner) + toward:
        pl.semaphore_signal(barrier, inc=1, device_id=target, device_id_type=MESH)
    pl.semaphore_wait(barrier, 4)

    tok = kv_in.shape[0]
    rows = wg_in.shape[0]
    units, lanes_down = wd_in.shape
    KV, GATE, UP, LOW, HIGH = range(5)

    def half(size, way, base=0):
        return pl.ds(base + way * (size // 2), size // 2)

    def part(start, size, way):
        return pl.ds(pl.multiple_of(start * size + way * (size // 2), size // 2), size // 2)

    def columns(o):
        return pl.ds(pl.multiple_of(o * lanes_down, lanes_down), lanes_down)

    ins = (
        lambda way: kv_in.at[half(tok, way), :],
        lambda way: wg_in.at[half(rows, way), :],
        lambda way: wu_in.at[half(rows, way), :],
        lambda way: wd_in.at[half(units // 2, way), :],
        lambda way: wd_in.at[half(units // 2, way, units // 2), :],
    )
    outs = (
        lambda o, way: kv_all.at[part(o, tok, way), :],
        lambda o, way: wg_all.at[part(o, rows, way), :],
        lambda o, way: wu_all.at[part(o, rows, way), :],
        lambda o, way: wd_all.at[half(units // 2, way), columns(o)],
        lambda o, way: wd_all.at[half(units // 2, way, units // 2), columns(o)],
    )
    own_outs = (
        kv_all.at[pl.ds(pl.multiple_of(sp * tok, tok), tok), :],
        wg_all.at[pl.ds(pl.multiple_of(sp * rows, rows), rows), :],
        wu_all.at[pl.ds(pl.multiple_of(sp * rows, rows), rows), :],
        wd_all.at[:, columns(sp)],
        wo_own,
    )
    own = [
        pltpu.make_async_copy(src, dst, own_sem.at[i])
        for i, (src, dst) in enumerate(zip((kv_in, wg_in, wu_in, wd_in, wo_in), own_outs))
    ]

    def owner(step, way, c):
        return at_pos(pos - step if way == 0 else pos + step, c)

    def remote(src, dst, send_sem, recv_sem, target):
        return pltpu.make_async_remote_copy(
            src_ref=src, dst_ref=dst, send_sem=send_sem, recv_sem=recv_sem,
            device_id=target, device_id_type=MESH,
        )

    def ring(kind, step, way):
        o = owner(step, way, core)
        src = ins[kind](way) if step == 0 else outs[kind](o, way)
        return remote(
            src, outs[kind](o, way),
            ring_send.at[kind, step, way], ring_recv.at[kind, step, way], toward[way],
        )

    def arrived(kind, step, way):
        piece = outs[kind](owner(step + 1, way, core), way)
        remote(
            piece, piece,
            ring_send.at[kind, step, way], ring_recv.at[kind, step, way], toward[way],
        ).wait_recv()

    def across(kind, step, way):
        o = owner(step, way, core)
        src = ins[kind](way) if step == 0 else outs[kind](o, way)
        return remote(
            src, outs[kind](o, way),
            sib_send.at[kind, step, way], sib_recv.at[kind, step, way], sibling,
        )

    def serve(kind, step):
        for way in range(2):
            if step > 0:
                arrived(kind, step - 1, way)
            if step < n - 1:
                ring(kind, step, way).start()
            across(kind, step, way).start()

    def sibling_gave(kind, steps):
        for step in steps:
            for way in range(2):
                piece = outs[kind](owner(step, way, 1 - core), way)
                remote(
                    piece, piece,
                    sib_send.at[kind, step, way], sib_recv.at[kind, step, way], sibling,
                ).wait_recv()

    pairs, q_rows, lanes = q_ref.shape
    block = math.gcd(q_rows, 256)
    per_pair = q_rows // block

    def attend(at):
        pair, which = at // per_pair, at % per_pair
        span = slice(which * block, (which + 1) * block)
        q = q_ref[pair, span, :]
        k = kv_all[:, pair * lanes:(pair + 1) * lanes]
        v = kv_all[:, (pairs + pair) * lanes:(pairs + pair + 1) * lanes]
        scores = lax.dot_general(
            q, k, (((1,), (1,)), ((), ())), preferred_element_type=jnp.float32
        )
        weights = jnp.exp(scores - jnp.max(scores, axis=-1, keepdims=True))
        total = jnp.sum(weights, axis=-1, keepdims=True)
        mixed = jnp.dot(weights.astype(jnp.bfloat16), v, preferred_element_type=jnp.float32)
        attn[pair, span, :] = (mixed / total).astype(jnp.bfloat16)

    width = wo_in.shape[1]

    def assemble():
        group = q_rows // (2 * tok)
        blocks = []
        for pair in range(pairs):
            for side in range(2):
                for g in range(0, group, 2):
                    lower = attn[pair, pl.ds((side * group + g) * tok, tok), :].astype(jnp.float32)
                    upper = attn[pair, pl.ds((side * group + g + 1) * tok, tok), :].astype(jnp.float32)
                    if side == 1:
                        lower = pltpu.roll(lower, head_size, 1)
                    else:
                        upper = pltpu.roll(upper, head_size, 1)
                    lane = lax.broadcasted_iota(jnp.int32, lower.shape, 1)
                    blocks.append(jnp.where(lane < head_size, lower, upper).astype(jnp.bfloat16))
        context[...] = jnp.concatenate(blocks, axis=1)

    own_count = res_ref.shape[0]
    mine = pl.ds(pl.multiple_of(tp * own_count, own_count), own_count)
    theirs = pl.ds(pl.multiple_of((1 - tp) * own_count, own_count), own_count)
    give_context = remote(context.at[theirs, :], context_in, x_send.at[0], x_recv.at[0], partner)
    give_wo = remote(wo_in, wo_other, x_send.at[2 + n], x_recv.at[2 + n], partner)
    give_normed = remote(
        normed.at[mine, :], normed.at[mine, :], x_send.at[1], x_recv.at[1], partner
    )
    take_normed = remote(
        normed.at[theirs, :], normed.at[theirs, :], x_send.at[1], x_recv.at[1], partner
    )

    def normalize():
        give_context.wait_recv()
        give_wo.wait_recv()
        own[4].wait()
        held, other = context[mine, :], context_in[...]
        wide = math.gcd(width, 512)
        for at in range(0, width, wide):
            cols = slice(at, at + wide)
            mid[:, cols] = res_ref[:, cols].astype(jnp.float32) + (
                jnp.dot(held, wo_own[:, cols], preferred_element_type=jnp.float32)
                + jnp.dot(other, wo_other[:, cols], preferred_element_type=jnp.float32)
            )
        value = mid[...]
        scale = lax.rsqrt(jnp.mean(value * value, axis=-1, keepdims=True) + EPS)
        normed[mine, :] = (value * scale * gain_ref[...]).astype(jnp.bfloat16)

    tile = math.gcd(units, 256)

    def feed(first, last):
        @pl.loop(first, last)
        def _(at):
            cols = pl.ds(pl.multiple_of(at * tile, tile), tile)
            x = normed[...]
            gate = jnp.dot(x, wg_all[:, cols], preferred_element_type=jnp.float32)
            up = jnp.dot(x, wu_all[:, cols], preferred_element_type=jnp.float32)
            hidden[:, cols] = (gate / (1.0 + jnp.exp(-gate)) * up).astype(jnp.bfloat16)

    def pair_columns(d):
        o = at_pos(pos - d, 0)
        return pl.ds(pl.multiple_of(o * lanes_down, 2 * lanes_down), 2 * lanes_down)

    def give_terms(d):
        return remote(leaving.at[d], coming.at[d], x_send.at[2 + d], x_recv.at[2 + d], partner)

    def lower(d):
        terms[...] = jnp.dot(
            hidden[...], wd_all[:, pair_columns(d)], preferred_element_type=jnp.float32
        )
        kept[d] = terms[mine, :]
        leaving[d] = terms[theirs, :].astype(jnp.bfloat16)

    def emit(d):
        give_terms(d).wait_recv()
        cols = pair_columns(d)
        down = kept[d] + coming[d].astype(jnp.float32)
        out_ref[:, cols] = (mid[:, cols] + 0.5 * down).astype(jnp.bfloat16)

    for copy in own:
        copy.start()
    early = [(kind, step) for step in range(n) for kind in (GATE, UP)]
    blocks = pairs * per_pair
    done_blocks = 0
    for slot, (kind, step) in enumerate(early):
        if slot < n:
            serve(KV, slot)
        serve(kind, step)
        if slot == 1:
            give_wo.start()
        if slot == 2 * n - 3:
            for ahead in (LOW, HIGH):
                serve(ahead, 0)
        if slot == n:
            own[KV].wait()
            sibling_gave(KV, range(n))
        if slot >= n:
            target = min(blocks, -(-blocks * (slot - n + 1) // (n - 2)))
            while done_blocks < target:
                attend(done_blocks)
                done_blocks += 1
        if slot == 2 * n - 3:
            assemble()
        if slot == 2 * n - 2:
            give_context.start()
        if slot == 2 * n - 1:
            normalize()
    tiles = units // tile
    fed = 0
    feed_from, feed_slots = 5, n - 5
    stage_of = {n // 2 + i: ([n // 2 - i, n // 2 + i] if i else [n // 2]) for i in range(n // 2)}
    waiting = []
    late = [(kind, step) for step in range(n) for kind in (LOW, HIGH)]
    for slot, (kind, step) in enumerate(late):
        if step > 0:
            serve(kind, step)
        for d in waiting:
            give_terms(d).start()
        waiting = []
        if slot == 2:
            give_normed.start()
            for other in (GATE, UP):
                own[other].wait()
                sibling_gave(other, range(n))
        if slot == feed_from - 1:
            take_normed.wait_recv()
        if feed_from - 1 <= slot < n:
            target = min(tiles, -(-tiles * (slot - feed_from + 2) // (feed_slots + 1)))
            if target > fed:
                feed(fed, target)
                fed = target
        if slot == n:
            own[3].wait()
            for other in (LOW, HIGH):
                sibling_gave(other, range(1))
            lower(0)
            waiting.append(0)
        if kind == HIGH and step >= n // 2:
            fresh = range(1, step + 1) if step == n // 2 else range(step, step + 1)
            for other in (LOW, HIGH):
                sibling_gave(other, fresh)
            for d in stage_of[step]:
                lower(d)
                waiting.append(d)
    give_terms(waiting[0]).start()
    ready = [0] + [d for step in range(n // 2, n - 1) for d in stage_of[step]]
    for d in ready:
        emit(d)
    give_terms(waiting[1]).start()
    for d in waiting:
        emit(d)
    for kind in range(5):
        for step in range(n):
            for way in range(2):
                if step < n - 1:
                    ring(kind, step, way).wait_send()
                across(kind, step, way).wait_send()
    give_context.wait_send()
    give_wo.wait_send()
    give_normed.wait_send()
    for d in range(n):
        give_terms(d).wait_send()


def fast_body(depth, queries, keys, values, q_gain, k_gain, w_out, residual, norm_gain, w_gate, w_up, w_down):
    tok_rows = queries.shape[0]
    head_size = q_gain.shape[0]
    q_heads = queries.shape[1] // head_size
    kv_heads = keys.shape[1] // head_size
    q_group = q_heads // kv_heads
    n_sp = 4 * depth
    positions = lax.axis_index("sp") * tok_rows + jnp.arange(tok_rows, dtype=jnp.int32)
    half_size = head_size // 2
    inv_freq = THETA ** (-jnp.arange(0, half_size, 2, dtype=jnp.float32) / half_size)
    row_angle = (positions // GRID_W).astype(jnp.float32)[:, None] * inv_freq[None, :]
    col_angle = (positions % GRID_W).astype(jnp.float32)[:, None] * inv_freq[None, :]
    angle = jnp.concatenate([row_angle, row_angle, col_angle, col_angle] * 2, axis=1)
    cos_table, sin_table = jnp.cos(angle), jnp.sin(angle)
    q_rot, k_rot = pl.pallas_call(
        functools.partial(rope_kernel, head_size),
        out_shape=(
            jax.ShapeDtypeStruct(queries.shape, jnp.bfloat16),
            jax.ShapeDtypeStruct(keys.shape, jnp.bfloat16),
        ),
        name="rope",
    )(
        queries, keys,
        q_gain[None, :], k_gain[None, :],
        cos_table, sin_table,
    )
    pairs = kv_heads // 2
    grouped = q_rot.reshape(tok_rows, pairs, 2, q_group, head_size)
    grouped = jnp.transpose(grouped, (1, 2, 3, 0, 4))
    empty = jnp.zeros_like(grouped[:, 0])
    padded = jnp.stack(
        [
            jnp.concatenate([grouped[:, 0], empty], axis=-1),
            jnp.concatenate([empty, grouped[:, 1]], axis=-1),
        ],
        axis=1,
    ).reshape(pairs, 2 * q_group * tok_rows, 2 * head_size)
    kv = jnp.concatenate([k_rot, values], axis=1)
    tokens = n_sp * tok_rows
    any_space = pl.BlockSpec(memory_space=pl.ANY)
    vmem = pl.BlockSpec(memory_space=pltpu.VMEM)
    n = 2 * depth
    own_count, width = residual.shape
    depth_in, units = w_gate.shape
    lanes_down = w_down.shape[1]
    bf16, f32 = jnp.bfloat16, jnp.float32
    return pl.pallas_call(
        functools.partial(layer_kernel, depth, head_size),
        out_shape=jax.ShapeDtypeStruct(residual.shape, bf16),
        in_specs=[vmem] * 4 + [any_space] * 4,
        out_specs=vmem,
        scratch_shapes=[
            pltpu.VMEM((tokens, kv.shape[1]), bf16),
            pltpu.VMEM((n_sp * depth_in, units), bf16),
            pltpu.VMEM((n_sp * depth_in, units), bf16),
            pltpu.VMEM((units, n_sp * lanes_down), bf16),
            pltpu.VMEM(w_out.shape, bf16),
            pltpu.VMEM(w_out.shape, bf16),
            pltpu.VMEM(padded.shape, bf16),
            pltpu.VMEM(queries.shape, bf16),
            pltpu.VMEM((own_count, queries.shape[1]), bf16),
            pltpu.VMEM((own_count, width), f32),
            pltpu.VMEM((tok_rows, width), bf16),
            pltpu.VMEM((tok_rows, units), bf16),
            pltpu.VMEM((tok_rows, 2 * lanes_down), f32),
            pltpu.VMEM((n, own_count, 2 * lanes_down), f32),
            pltpu.VMEM((n, own_count, 2 * lanes_down), bf16),
            pltpu.VMEM((n, own_count, 2 * lanes_down), bf16),
            pltpu.SemaphoreType.DMA((5,)),
            pltpu.SemaphoreType.DMA((5, n - 1, 2)),
            pltpu.SemaphoreType.DMA((5, n - 1, 2)),
            pltpu.SemaphoreType.DMA((5, n, 2)),
            pltpu.SemaphoreType.DMA((5, n, 2)),
            pltpu.SemaphoreType.DMA((3 + n,)),
            pltpu.SemaphoreType.DMA((3 + n,)),
        ],
        compiler_params=pltpu.CompilerParams(
            collective_id=0, has_side_effects=True, vmem_limit_bytes=63 * 1024 * 1024
        ),
        name="layer",
    )(padded, kv, residual, norm_gain[None, :], w_out, w_gate, w_up, w_down)


def solution(mesh):
    depth = physical_ring(mesh)
    inner = body if depth is None else functools.partial(fast_body, depth)
    return jax.shard_map(
        inner,
        mesh=mesh,
        in_specs=(
            P("sp", "tp"),
            P("sp", "tp"),
            P("sp", "tp"),
            P(),
            P(),
            P("tp", None),
            P(("sp", "tp"), None),
            P(),
            P("sp", "tp"),
            P("sp", "tp"),
            P("tp", "sp"),
        ),
        out_specs=P(("sp", "tp"), None),
        check_vma=False,
    )
```

```python
import functools
import math

import jax
import jax.numpy as jnp
from jax import lax
from jax.experimental import pallas as pl
from jax.experimental.pallas import tpu as pltpu
from jax.sharding import PartitionSpec as P

GRID_W = 128


EPS = 1e-06
THETA = 10000.0


def turn_half(part, angle):
    quarter = part.shape[-1] // 2
    cos_table = jnp.cos(angle)[:, None, :]
    sin_table = jnp.sin(angle)[:, None, :]
    first_part = part[..., :quarter]
    second_part = part[..., quarter:]
    return jnp.concatenate(
        [
            first_part * cos_table - second_part * sin_table,
            first_part * sin_table + second_part * cos_table,
        ],
        axis=-1,
    )


def head_norm_rope(flat, gain, offset, head_count):
    tok_rows = flat.shape[0]
    head_size = flat.shape[1] // head_count
    heads = flat.astype(jnp.float32).reshape(tok_rows, head_count, head_size)
    heads = heads * lax.rsqrt(jnp.mean(heads * heads, axis=-1, keepdims=True) + EPS) * gain
    positions = offset + jnp.arange(tok_rows, dtype=jnp.int32)
    row_pos = (positions // GRID_W).astype(jnp.float32)
    col_pos = (positions % GRID_W).astype(jnp.float32)
    half_size = head_size // 2
    inv_freq = THETA ** (-jnp.arange(0, half_size, 2, dtype=jnp.float32) / half_size)
    turned = jnp.concatenate(
        [
            turn_half(heads[..., :half_size], row_pos[:, None] * inv_freq[None, :]),
            turn_half(heads[..., half_size:], col_pos[:, None] * inv_freq[None, :]),
        ],
        axis=-1,
    )
    return turned.reshape(tok_rows, head_count * head_size).astype(jnp.bfloat16)


def body(queries, keys, values, q_gain, k_gain, w_out, residual, norm_gain, w_gate, w_up, w_down):
    tok_rows = queries.shape[0]
    head_size = q_gain.shape[0]
    q_heads = queries.shape[1] // head_size
    kv_heads = keys.shape[1] // head_size
    q_group = q_heads // kv_heads
    offset = lax.axis_index("sp") * tok_rows
    q_rot = head_norm_rope(queries, q_gain, offset, q_heads)
    k_rot = head_norm_rope(keys, k_gain, offset, kv_heads)
    query_groups = q_rot.reshape(tok_rows, kv_heads, q_group, head_size)
    score_scale = head_size ** (-0.5)
    start_state = (
        jnp.full((kv_heads, q_group, tok_rows), -1e30, jnp.float32),
        jnp.zeros((kv_heads, q_group, tok_rows), jnp.float32),
        jnp.zeros((kv_heads, q_group, tok_rows, head_size), jnp.float32),
    )
    running = start_state
    key_piece = lax.all_gather(k_rot, "sp", axis=0, tiled=True)
    value_piece = lax.all_gather(values, "sp", axis=0, tiled=True)
    piece_len = key_piece.shape[0]
    block_len = math.gcd(piece_len, 512)
    blocks = piece_len // block_len
    key_blocks = key_piece.reshape(blocks, block_len, kv_heads, head_size)
    value_blocks = value_piece.reshape(blocks, block_len, kv_heads, head_size)

    def update(state, block_pair):
        prior_max, totals, accum = state
        key_block, value_block = block_pair
        scores = (
            jnp.einsum(
                "qhgd,khd->hgqk", query_groups, key_block, preferred_element_type=jnp.float32
            )
            * score_scale
        )
        new_max = jnp.maximum(prior_max, jnp.max(scores, axis=-1))
        weights = jnp.exp(scores - new_max[..., None])
        factor = jnp.exp(prior_max - new_max)
        totals = totals * factor + jnp.sum(weights, axis=-1)
        accum = accum * factor[..., None] + jnp.einsum(
            "hgqk,khd->hgqd",
            weights.astype(jnp.bfloat16),
            value_block,
            preferred_element_type=jnp.float32,
        )
        return ((new_max, totals, accum), None)

    running, unused = lax.scan(update, running, (key_blocks, value_blocks))
    final_max, totals, accum = running
    mixed = accum / totals[..., None]
    attn = (
        jnp.transpose(mixed, (2, 0, 1, 3))
        .reshape(tok_rows, q_heads * head_size)
        .astype(jnp.bfloat16)
    )
    own_rows = lax.all_to_all(attn, "tp", split_axis=0, concat_axis=1, tiled=True)
    columns = own_rows
    proj = jnp.dot(
        columns, lax.all_gather(w_out, "tp", axis=0, tiled=True), preferred_element_type=jnp.float32
    )
    mid = residual.astype(jnp.float32) + proj
    normed = (
        mid * lax.rsqrt(jnp.mean(mid * mid, axis=-1, keepdims=True) + EPS) * norm_gain
    ).astype(jnp.bfloat16)
    gathered = lax.all_gather(normed, "tp", axis=0, tiled=True)
    columns = gathered
    gate = jnp.dot(
        columns,
        lax.all_gather(w_gate, "sp", axis=0, tiled=True),
        preferred_element_type=jnp.float32,
    )
    up_part = jnp.dot(
        columns, lax.all_gather(w_up, "sp", axis=0, tiled=True), preferred_element_type=jnp.float32
    )
    hidden = (jax.nn.silu(gate) * up_part).astype(jnp.bfloat16)
    terms = jnp.dot(
        hidden, lax.all_gather(w_down, "sp", axis=1, tiled=True), preferred_element_type=jnp.float32
    )
    down = lax.psum_scatter(
        terms.astype(jnp.bfloat16), "tp", scatter_dimension=0, tiled=True
    ).astype(jnp.float32)
    return (mid + 0.5 * down).astype(jnp.bfloat16)


MESH = pl.DeviceIdType.MESH


def physical_ring(mesh):
    count = mesh.shape["sp"]
    try:
        places = [(tuple(d.coords), d.core_on_chip) for d in mesh.devices[:, 0].flat]
    except AttributeError:
        return None
    if count % 4 or count < 12 or mesh.shape["tp"] != 2:
        return None
    first = places[0][0]
    depth = count // 4
    for at, (coords, core) in enumerate(places):
        chip = at // 2
        want = (first[0], first[1] + chip % 2, first[2] + chip // 2)
        if coords != want or core != at % 2:
            return None
    return depth


def turned_heads(head_size, x_ref, g_ref, cos_ref, sin_ref):
    x = x_ref[...].astype(jnp.float32)
    width = x.shape[1]
    lane = lax.broadcasted_iota(jnp.int32, (width, width), 0) // head_size
    other = lax.broadcasted_iota(jnp.int32, (width, width), 1) // head_size
    same = (lane == other).astype(jnp.float32)
    mean = jnp.dot(
        x * x, same, preferred_element_type=jnp.float32, precision=lax.Precision.HIGHEST
    ) * (1.0 / head_size)
    h = x * lax.rsqrt(mean + EPS) * jnp.concatenate([g_ref[...]] * (width // head_size), axis=1)
    quarter = head_size // 4
    repeats = width // cos_ref.shape[1]
    cos_table = jnp.concatenate([cos_ref[...]] * repeats, axis=1)
    sin_table = jnp.concatenate([sin_ref[...]] * repeats, axis=1)
    at = lax.broadcasted_iota(jnp.int32, x.shape, 1)
    is_first = (at // quarter) % 2 == 0
    ahead = pltpu.roll(h, width - quarter, 1)
    behind = pltpu.roll(h, quarter, 1)
    turned = h * cos_table + jnp.where(is_first, -ahead, behind) * sin_table
    return turned.astype(jnp.bfloat16)


def layer_kernel(
    depth, head_size,
    raw_q, raw_k, raw_v, qg_ref, kg_ref, cos_ref, sin_ref, res_ref, gain_ref, wo_in, wg_in, wu_in, wd_in,
    out_ref,
    q_ref, kv_in, kv_all, wg_all, wu_all, wd_all, wo_own, wo_other, attn, context, context_in, mid, normed, hidden,
    terms, kept, leaving, coming,
    own_sem, ring_send, ring_recv, sib_send, sib_recv, x_send, x_recv,
):
    n = 2 * depth
    sp = lax.axis_index("sp")
    tp = lax.axis_index("tp")
    core = sp % 2
    z = sp // 4
    y = (sp // 2) % 2
    pos = (1 - y) * z + y * (n - 1 - z)

    def at_pos(p, c):
        p = lax.rem(p + n, n)
        yy = p // depth
        zz = (1 - yy) * p + yy * (n - 1 - p)
        return (zz * 2 + yy) * 2 + c

    sibling = (at_pos(pos, 1 - core), tp)
    partner = (sp, 1 - tp)
    toward = ((at_pos(pos + 1, core), tp), (at_pos(pos - 1, core), tp))

    barrier = pltpu.get_barrier_semaphore()
    for target in (sibling, partner) + toward:
        pl.semaphore_signal(barrier, inc=1, device_id=target, device_id_type=MESH)
    pl.semaphore_wait(barrier, 4)

    tok = kv_in.shape[0]
    rows = wg_in.shape[0]
    units, lanes_down = wd_in.shape
    KV, GATE, UP, LOW, HIGH = range(5)

    def half(size, way, base=0):
        return pl.ds(base + way * (size // 2), size // 2)

    def part(start, size, way):
        return pl.ds(pl.multiple_of(start * size + way * (size // 2), size // 2), size // 2)

    def columns(o):
        return pl.ds(pl.multiple_of(o * lanes_down, lanes_down), lanes_down)

    ins = (
        lambda way: kv_in.at[half(tok, way), :],
        lambda way: wg_in.at[half(rows, way), :],
        lambda way: wu_in.at[half(rows, way), :],
        lambda way: wd_in.at[half(units // 2, way), :],
        lambda way: wd_in.at[half(units // 2, way, units // 2), :],
    )
    outs = (
        lambda o, way: kv_all.at[part(o, tok, way), :],
        lambda o, way: wg_all.at[part(o, rows, way), :],
        lambda o, way: wu_all.at[part(o, rows, way), :],
        lambda o, way: wd_all.at[half(units // 2, way), columns(o)],
        lambda o, way: wd_all.at[half(units // 2, way, units // 2), columns(o)],
    )
    own_outs = (
        kv_all.at[pl.ds(pl.multiple_of(sp * tok, tok), tok), :],
        wg_all.at[pl.ds(pl.multiple_of(sp * rows, rows), rows), :],
        wu_all.at[pl.ds(pl.multiple_of(sp * rows, rows), rows), :],
        wd_all.at[:, columns(sp)],
        wo_own,
    )
    own = [
        pltpu.make_async_copy(src, dst, own_sem.at[i])
        for i, (src, dst) in enumerate(zip((kv_in, wg_in, wu_in, wd_in, wo_in), own_outs))
    ]

    def owner(step, way, c):
        return at_pos(pos - step if way == 0 else pos + step, c)

    def remote(src, dst, send_sem, recv_sem, target):
        return pltpu.make_async_remote_copy(
            src_ref=src, dst_ref=dst, send_sem=send_sem, recv_sem=recv_sem,
            device_id=target, device_id_type=MESH,
        )

    def ring(kind, step, way):
        o = owner(step, way, core)
        src = ins[kind](way) if step == 0 else outs[kind](o, way)
        return remote(
            src, outs[kind](o, way),
            ring_send.at[kind, step, way], ring_recv.at[kind, step, way], toward[way],
        )

    def arrived(kind, step, way):
        piece = outs[kind](owner(step + 1, way, core), way)
        remote(
            piece, piece,
            ring_send.at[kind, step, way], ring_recv.at[kind, step, way], toward[way],
        ).wait_recv()

    def across(kind, step, way):
        o = owner(step, way, core)
        src = ins[kind](way) if step == 0 else outs[kind](o, way)
        return remote(
            src, outs[kind](o, way),
            sib_send.at[kind, step, way], sib_recv.at[kind, step, way], sibling,
        )

    def serve(kind, step):
        for way in range(2):
            if step > 0:
                arrived(kind, step - 1, way)
            if step < n - 1:
                ring(kind, step, way).start()
            across(kind, step, way).start()

    def sibling_gave(kind, steps):
        for step in steps:
            for way in range(2):
                piece = outs[kind](owner(step, way, 1 - core), way)
                remote(
                    piece, piece,
                    sib_send.at[kind, step, way], sib_recv.at[kind, step, way], sibling,
                ).wait_recv()

    pairs, q_rows, lanes = q_ref.shape
    block = math.gcd(q_rows, 256)
    per_pair = q_rows // block

    def attend(at):
        pair, which = at // per_pair, at % per_pair
        span = slice(which * block, (which + 1) * block)
        q = q_ref[pair, span, :]
        k = kv_all[:, pair * lanes:(pair + 1) * lanes]
        v = kv_all[:, (pairs + pair) * lanes:(pairs + pair + 1) * lanes]
        scores = lax.dot_general(
            q, k, (((1,), (1,)), ((), ())), preferred_element_type=jnp.float32
        )
        weights = jnp.exp(scores - jnp.max(scores, axis=-1, keepdims=True))
        total = jnp.sum(weights, axis=-1, keepdims=True)
        mixed = jnp.dot(weights.astype(jnp.bfloat16), v, preferred_element_type=jnp.float32)
        attn[pair, span, :] = (mixed / total).astype(jnp.bfloat16)

    width = wo_in.shape[1]

    def assemble():
        group = q_rows // (2 * tok)
        blocks = []
        for pair in range(pairs):
            for side in range(2):
                for g in range(0, group, 2):
                    lower = attn[pair, pl.ds((side * group + g) * tok, tok), :].astype(jnp.float32)
                    upper = attn[pair, pl.ds((side * group + g + 1) * tok, tok), :].astype(jnp.float32)
                    if side == 1:
                        lower = pltpu.roll(lower, head_size, 1)
                    else:
                        upper = pltpu.roll(upper, head_size, 1)
                    lane = lax.broadcasted_iota(jnp.int32, lower.shape, 1)
                    blocks.append(jnp.where(lane < head_size, lower, upper).astype(jnp.bfloat16))
        context[...] = jnp.concatenate(blocks, axis=1)

    own_count = res_ref.shape[0]
    mine = pl.ds(pl.multiple_of(tp * own_count, own_count), own_count)
    theirs = pl.ds(pl.multiple_of((1 - tp) * own_count, own_count), own_count)
    give_context = remote(context.at[theirs, :], context_in, x_send.at[0], x_recv.at[0], partner)
    give_wo = remote(wo_in, wo_other, x_send.at[2 + n], x_recv.at[2 + n], partner)
    give_normed = remote(
        normed.at[mine, :], normed.at[mine, :], x_send.at[1], x_recv.at[1], partner
    )
    take_normed = remote(
        normed.at[theirs, :], normed.at[theirs, :], x_send.at[1], x_recv.at[1], partner
    )

    def normalize():
        give_context.wait_recv()
        give_wo.wait_recv()
        own[4].wait()
        held, other = context[mine, :], context_in[...]
        wide = math.gcd(width, 512)
        for at in range(0, width, wide):
            cols = slice(at, at + wide)
            mid[:, cols] = res_ref[:, cols].astype(jnp.float32) + (
                jnp.dot(held, wo_own[:, cols], preferred_element_type=jnp.float32)
                + jnp.dot(other, wo_other[:, cols], preferred_element_type=jnp.float32)
            )
        value = mid[...]
        scale = lax.rsqrt(jnp.mean(value * value, axis=-1, keepdims=True) + EPS)
        normed[mine, :] = (value * scale * gain_ref[...]).astype(jnp.bfloat16)

    tile = math.gcd(units, 256)

    def feed(first, last):
        @pl.loop(first, last)
        def _(at):
            cols = pl.ds(pl.multiple_of(at * tile, tile), tile)
            x = normed[...]
            gate = jnp.dot(x, wg_all[:, cols], preferred_element_type=jnp.float32)
            up = jnp.dot(x, wu_all[:, cols], preferred_element_type=jnp.float32)
            hidden[:, cols] = (gate / (1.0 + jnp.exp(-gate)) * up).astype(jnp.bfloat16)

    def pair_columns(d):
        o = at_pos(pos - d, 0)
        return pl.ds(pl.multiple_of(o * lanes_down, 2 * lanes_down), 2 * lanes_down)

    def give_terms(d):
        return remote(leaving.at[d], coming.at[d], x_send.at[2 + d], x_recv.at[2 + d], partner)

    def lower(d):
        terms[...] = jnp.dot(
            hidden[...], wd_all[:, pair_columns(d)], preferred_element_type=jnp.float32
        )
        kept[d] = terms[mine, :]
        leaving[d] = terms[theirs, :].astype(jnp.bfloat16)

    def emit(d):
        give_terms(d).wait_recv()
        cols = pair_columns(d)
        down = kept[d] + coming[d].astype(jnp.float32)
        out_ref[:, cols] = (mid[:, cols] + 0.5 * down).astype(jnp.bfloat16)

    for copy in own[1:]:
        copy.start()
    serve(GATE, 0)
    k_width = raw_k.shape[1]
    kv_in[:, :k_width] = turned_heads(head_size, raw_k, kg_ref, cos_ref, sin_ref)
    kv_in[:, k_width:] = raw_v[...]
    turned = turned_heads(head_size, raw_q, qg_ref, cos_ref, sin_ref).astype(jnp.float32)
    turned = turned * head_size ** (-0.5)
    group = q_rows // (2 * tok)
    for at in range(raw_q.shape[1] // lanes):
        both = turned[:, at * lanes:(at + 1) * lanes]
        swapped = pltpu.roll(both, head_size, 1)
        low = lax.broadcasted_iota(jnp.int32, both.shape, 1) < head_size
        key_head, g = 2 * at // group, 2 * at % group
        pair, side = key_head // 2, key_head % 2
        for extra in range(2):
            source = both if extra == side else swapped
            kept_lanes = jnp.where(low if side == 0 else jnp.logical_not(low), source, 0.0)
            first = (side * group + g + extra) * tok
            q_ref[pair, first:first + tok, :] = kept_lanes.astype(jnp.bfloat16)
    own[KV].start()
    early = [(kind, step) for step in range(n) for kind in (GATE, UP)]
    blocks = pairs * per_pair
    done_blocks = 0
    for slot, (kind, step) in enumerate(early):
        if slot < n:
            serve(KV, slot)
        if slot > 0:
            serve(kind, step)
        if slot == 1:
            give_wo.start()
        if slot == 2 * n - 3:
            for ahead in (LOW, HIGH):
                serve(ahead, 0)
        if slot == n:
            own[KV].wait()
            sibling_gave(KV, range(n))
        if slot >= n:
            target = min(blocks, -(-blocks * (slot - n + 1) // (n - 2)))
            while done_blocks < target:
                attend(done_blocks)
                done_blocks += 1
        if slot == 2 * n - 3:
            assemble()
        if slot == 2 * n - 2:
            give_context.start()
        if slot == 2 * n - 1:
            normalize()
    tiles = units // tile
    fed = 0
    feed_from, feed_slots = 5, n - 5
    stage_of = {n // 2 + i: ([n // 2 - i, n // 2 + i] if i else [n // 2]) for i in range(n // 2)}
    waiting = []
    late = [(kind, step) for step in range(n) for kind in (LOW, HIGH)]
    for slot, (kind, step) in enumerate(late):
        if step > 0:
            serve(kind, step)
        for d in waiting:
            give_terms(d).start()
        waiting = []
        if slot == 2:
            give_normed.start()
            for other in (GATE, UP):
                own[other].wait()
                sibling_gave(other, range(n))
        if slot == feed_from - 1:
            take_normed.wait_recv()
        if feed_from - 1 <= slot < n:
            target = min(tiles, -(-tiles * (slot - feed_from + 2) // (feed_slots + 1)))
            if target > fed:
                feed(fed, target)
                fed = target
        if slot == n:
            own[3].wait()
            for other in (LOW, HIGH):
                sibling_gave(other, range(1))
            lower(0)
            waiting.append(0)
        if kind == HIGH and step >= n // 2:
            fresh = range(1, step + 1) if step == n // 2 else range(step, step + 1)
            for other in (LOW, HIGH):
                sibling_gave(other, fresh)
            for d in stage_of[step]:
                lower(d)
                waiting.append(d)
    give_terms(waiting[0]).start()
    ready = [0] + [d for step in range(n // 2, n - 1) for d in stage_of[step]]
    for d in ready:
        emit(d)
    give_terms(waiting[1]).start()
    for d in waiting:
        emit(d)
    for kind in range(5):
        for step in range(n):
            for way in range(2):
                if step < n - 1:
                    ring(kind, step, way).wait_send()
                across(kind, step, way).wait_send()
    give_context.wait_send()
    give_wo.wait_send()
    give_normed.wait_send()
    for d in range(n):
        give_terms(d).wait_send()


def fast_body(depth, queries, keys, values, q_gain, k_gain, w_out, residual, norm_gain, w_gate, w_up, w_down):
    tok_rows = queries.shape[0]
    head_size = q_gain.shape[0]
    q_heads = queries.shape[1] // head_size
    kv_heads = keys.shape[1] // head_size
    q_group = q_heads // kv_heads
    n_sp = 4 * depth
    positions = lax.axis_index("sp") * tok_rows + jnp.arange(tok_rows, dtype=jnp.int32)
    half_size = head_size // 2
    inv_freq = THETA ** (-jnp.arange(0, half_size, 2, dtype=jnp.float32) / half_size)
    row_angle = (positions // GRID_W).astype(jnp.float32)[:, None] * inv_freq[None, :]
    col_angle = (positions % GRID_W).astype(jnp.float32)[:, None] * inv_freq[None, :]
    angle = jnp.concatenate([row_angle, row_angle, col_angle, col_angle] * 2, axis=1)
    cos_table, sin_table = jnp.cos(angle), jnp.sin(angle)
    pairs = kv_heads // 2
    padded = (pairs, 2 * q_group * tok_rows, 2 * head_size)
    kv_shape = (tok_rows, keys.shape[1] + values.shape[1])
    tokens = n_sp * tok_rows
    any_space = pl.BlockSpec(memory_space=pl.ANY)
    vmem = pl.BlockSpec(memory_space=pltpu.VMEM)
    n = 2 * depth
    own_count, width = residual.shape
    depth_in, units = w_gate.shape
    lanes_down = w_down.shape[1]
    bf16, f32 = jnp.bfloat16, jnp.float32
    return pl.pallas_call(
        functools.partial(layer_kernel, depth, head_size),
        out_shape=jax.ShapeDtypeStruct(residual.shape, bf16),
        in_specs=[vmem] * 9 + [any_space] * 4,
        out_specs=vmem,
        scratch_shapes=[
            pltpu.VMEM(padded, bf16),
            pltpu.VMEM(kv_shape, bf16),
            pltpu.VMEM((tokens, kv_shape[1]), bf16),
            pltpu.VMEM((n_sp * depth_in, units), bf16),
            pltpu.VMEM((n_sp * depth_in, units), bf16),
            pltpu.VMEM((units, n_sp * lanes_down), bf16),
            pltpu.VMEM(w_out.shape, bf16),
            pltpu.VMEM(w_out.shape, bf16),
            pltpu.VMEM(padded, bf16),
            pltpu.VMEM(queries.shape, bf16),
            pltpu.VMEM((own_count, queries.shape[1]), bf16),
            pltpu.VMEM((own_count, width), f32),
            pltpu.VMEM((tok_rows, width), bf16),
            pltpu.VMEM((tok_rows, units), bf16),
            pltpu.VMEM((tok_rows, 2 * lanes_down), f32),
            pltpu.VMEM((n, own_count, 2 * lanes_down), f32),
            pltpu.VMEM((n, own_count, 2 * lanes_down), bf16),
            pltpu.VMEM((n, own_count, 2 * lanes_down), bf16),
            pltpu.SemaphoreType.DMA((5,)),
            pltpu.SemaphoreType.DMA((5, n - 1, 2)),
            pltpu.SemaphoreType.DMA((5, n - 1, 2)),
            pltpu.SemaphoreType.DMA((5, n, 2)),
            pltpu.SemaphoreType.DMA((5, n, 2)),
            pltpu.SemaphoreType.DMA((3 + n,)),
            pltpu.SemaphoreType.DMA((3 + n,)),
        ],
        compiler_params=pltpu.CompilerParams(
            collective_id=0, has_side_effects=True, vmem_limit_bytes=63 * 1024 * 1024
        ),
        name="layer",
    )(
        queries, keys, values, q_gain[None, :], k_gain[None, :], cos_table, sin_table,
        residual, norm_gain[None, :], w_out, w_gate, w_up, w_down)


def solution(mesh):
    depth = physical_ring(mesh)
    inner = body if depth is None else functools.partial(fast_body, depth)
    return jax.shard_map(
        inner,
        mesh=mesh,
        in_specs=(
            P("sp", "tp"),
            P("sp", "tp"),
            P("sp", "tp"),
            P(),
            P(),
            P("tp", None),
            P(("sp", "tp"), None),
            P(),
            P("sp", "tp"),
            P("sp", "tp"),
            P("tp", "sp"),
        ),
        out_specs=P(("sp", "tp"), None),
        check_vma=False,
    )
```
